32 devices in a mesh: grp: 2 (over x), ep: 16 (over z, y, core).
Axes of the slice: x: 2, y: 2, z: 4, core: 2. Of those that a mesh axis runs over, the one named last changes fastest.
Arguments:
- tokens: bfloat16 [16384, 2048], P(('grp', 'ep')), parts along dimension 0, may hold values from -6 to 6
- norm_gain: float32 [2048], replicated, may hold values from 0.1 to 1.9
- route_ids: int32 [16384, 2], P(('grp', 'ep')), parts along dimension 0, may hold values from 0 to 15, all different within a row; in each aligned block of 512 rows (0 to 511, 512 to 1023, ...) at most 96 rows name the same one
- route_gates: float32 [16384, 2], P(('grp', 'ep')), parts along dimension 0, may hold values from 0.05 to 1
- w_gate: bfloat16 [16, 2048, 1024], P('ep'), may hold values from -0.125 to 0.125
- w_up: bfloat16 [16, 2048, 1024], P('ep'), may hold values from -0.125 to 0.125
- w_down: bfloat16 [16, 1024, 2048], P('ep'), may hold values from -0.1875 to 0.1875
Outputs:
- mixed: bfloat16 [16384, 2048], P(('grp', 'ep')), parts along dimension 0
The draws below stay inside these ranges and needn't reach their ends.
There are 2 independent parts, one for each index of `grp`. The reference program is written for one: setup_inputs(seed, part) draws one part's arguments, and reference() takes and returns one part's arrays. A program takes and returns all parts, laid end to end along the dimension named above; an argument that names none is the same for every part. Nothing has to cross between parts.
Inputs may be any that keep to these rules, and one draw needn't show every extreme that they name: `route_ids`: each row names 2 different experts. Among the rows of one device no expert is named more than 96 times, and in some devices' rows one expert is named exactly 96 times.
All inputs are finite; a program needn't handle non-finite values.
Results may differ from the reference program's by a relative error of at most 0.0071.
Values may be sent and summed in bfloat16 or wider, within the bound.
A program may use at most 128 MiB of HBM per device.

```python
import math
import jax
import jax.numpy as jnp
import numpy as np
from jax import lax

D = 2048
FF = 1024
TOPK = 2
TOK_DEV = 512
EXPERTS = 16
CAP = 96
TOKENS = 8192
N_EP = 16


def steps_of(rng, dims, split, low, top_value):
    level = 1.0
    for axis_at, parts in split:
        draws = jax.random.uniform(jax.random.fold_in(jax.random.fold_in(rng, 6), axis_at), (parts,), jnp.float32, low / len(split), top_value / len(split))
        level = level * jnp.repeat(jnp.exp(draws), dims[axis_at] // parts).reshape((-1,) + (1,) * (len(dims) - 1 - axis_at))
    return level


def shared_out(key, own, number, rows, number_of, top, most, slope):
    sequence = jax.random.permutation(key, number_of)
    packed, common = shares(number_of, rows * top, most, slope, True), shares(number_of, rows * top, most, slope, False)
    places = jnp.arange(number_of)

    def named(lengths, offset_by):
        used = int((lengths > 0).sum())
        fixed = max(1, used // 4)
        shifted = fixed + (places - fixed + offset_by * (used - fixed)) % max(1, number_of - fixed)
        return jnp.zeros((number_of,), jnp.int32).at[sequence[jnp.where(places < fixed, places, shifted)]].set(jnp.asarray(lengths, jnp.int32))

    lengths = jnp.where(number % 4 == 0, named(packed, number // 4), named(common, number - number // 4 - 1))
    mixed = jax.random.permutation(jax.random.fold_in(own, 3), number_of)
    giver, sink = mixed[0:number_of // 2 * 2:2], mixed[1:number_of // 2 * 2:2]
    slack = jnp.minimum(lengths[giver] - 1, most - lengths[sink]) // 2
    slack = jnp.where((giver == sequence[0]) | (sink == sequence[0]) | (lengths[sink] == 0), 0, jnp.maximum(slack, 0))
    shifted = jax.random.randint(jax.random.fold_in(own, 4), (number_of // 2,), 0, 1 << 20) % (slack + 1)
    lengths = lengths.at[giver].add(-shifted).at[sink].add(shifted)
    labels = jnp.searchsorted(jnp.cumsum(lengths), jnp.arange(rows * top), side="right").astype(jnp.int32)
    listing = labels.reshape(top, rows).T
    listing = listing[jax.random.permutation(jax.random.fold_in(own, 1), rows)]
    offset_by = jax.random.randint(jax.random.fold_in(own, 2), (rows, 1), 0, top)
    return jnp.take_along_axis(listing, (jnp.arange(top)[None, :] + offset_by) % top, axis=1)


def shares(number_of, total, most, slope, full):
    weights = [(1 << 20) // math.isqrt(rank ** slope) + 1 for rank in range(1, number_of + 1)]
    largest = most if full else min(most, max(-(-total // number_of), total * weights[0] // sum(weights)))
    least = 1 if total - largest >= number_of - 1 else 0
    counts, rest = [largest] + [least] * (number_of - 1), total - largest - least * (number_of - 1)
    while rest > 0:
        movable = [i for i in range(1, number_of) if counts[i] < largest] or [i for i in range(1, number_of) if counts[i] < most]
        mass, remaining = sum([weights[i] for i in movable]), rest
        for i in movable:
            extra = min(most - counts[i], max(1, remaining * weights[i] // mass), rest)
            counts[i] = counts[i] + extra
            rest = rest - extra
    return np.array(counts)


def scatter_about(own_key, shape, spread, limit, shards=(), held_as=jnp.bfloat16):
    array = jax.random.normal(own_key, shape, jnp.float32) * spread
    if len(shards) > 0:
        array = steps_of(own_key, shape, shards, -0.22, 0.18) * array
    return jnp.clip(array, min=-limit, max=limit).astype(held_as)


def setup_inputs(seed: int = 0, part: int = 0) -> dict:
    streams_of = jax.random.split(jax.random.key(seed), 8)
    part_splits = jax.random.split(jax.random.fold_in(streams_of[7], part), 8)
    tokens = scatter_about(part_splits[0], (TOKENS, D), 1.0, 6.0, ((0, 16),))
    norm_gain = jnp.clip(1.0 + 0.18 * jax.random.normal(streams_of[1], (D,), jnp.float32), 0.1, 1.9)
    route_ids_keys = jax.random.split(jax.random.fold_in(part_splits[2], 1), TOKENS // TOK_DEV)
    route_ids_turns = jax.random.permutation(jax.random.fold_in(part_splits[2], 3), TOKENS // TOK_DEV)
    route_ids = jax.vmap(lambda own, number: shared_out(jax.random.fold_in(part_splits[2], 2), own, number, TOK_DEV, EXPERTS, TOPK, CAP, 2))(route_ids_keys, route_ids_turns).reshape((TOKENS, TOPK))
    route_gates = jnp.clip(0.05 + 0.95 * jax.random.uniform(part_splits[3], (TOKENS, TOPK), jnp.float32) ** steps_of(part_splits[3], (TOKENS, TOPK), ((0, 16),), -0.2, 0.2), 0.05, 1.0)
    w_gate = scatter_about(streams_of[4], (EXPERTS, D, FF), D ** -0.5, 0.125, ((0, 16),))
    w_up = scatter_about(streams_of[5], (EXPERTS, D, FF), D ** -0.5, 0.125, ((0, 16),))
    w_down = scatter_about(streams_of[6], (EXPERTS, FF, D), FF ** -0.5, 0.1875, ((0, 16),))
    return dict(tokens=tokens, norm_gain=norm_gain, route_ids=route_ids, route_gates=route_gates, w_gate=w_gate, w_up=w_up, w_down=w_down)


EPS = 1e-06

def reference(tokens, norm_gain, route_ids, route_gates, w_gate, w_up, w_down):
    floats = tokens.astype(jnp.float32)
    scale = lax.rsqrt(lax.optimization_barrier(jnp.mean(floats * floats, axis=-1, keepdims=True)) + EPS)
    normed = (floats * scale * norm_gain).astype(jnp.bfloat16)
    weights = route_gates / lax.optimization_barrier(jnp.sum(route_gates, axis=-1, keepdims=True))
    count = TOKENS * TOPK
    flat_ids = route_ids.reshape(-1)
    flat_weights = weights.reshape(-1)
    most = N_EP * CAP

    def one_expert(carry, inputs):
        expert, gate_mat, up_mat, down_mat = inputs
        picked = jnp.nonzero(flat_ids == expert, size=most, fill_value=count)[0].astype(jnp.int32)
        live = picked < count
        pairs = jnp.minimum(picked, count - 1)
        rows = pairs // TOPK
        chosen = normed[rows]
        gate_pre = jnp.dot(chosen, gate_mat, preferred_element_type=jnp.float32)
        up_pre = jnp.dot(chosen, up_mat, preferred_element_type=jnp.float32)
        hidden = (jax.nn.silu(gate_pre) * up_pre).astype(jnp.bfloat16)
        result = jnp.dot(hidden, down_mat, preferred_element_type=jnp.float32).astype(jnp.bfloat16)
        factor = jnp.where(live, flat_weights[pairs], jnp.zeros_like(flat_weights[pairs]))
        return (carry.at[rows].add(result.astype(jnp.float32) * factor[:, None]), None)
    start = jnp.zeros((TOKENS, D), jnp.float32)
    total, _ = lax.scan(one_expert, start, (jnp.arange(EXPERTS, dtype=jnp.int32), w_gate, w_up, w_down))
    return total.astype(jnp.bfloat16)
```

```python
import functools

import jax
import jax.numpy as jnp
from jax import lax
from jax.experimental import pallas as pl
from jax.experimental.pallas import tpu as pltpu
from jax.sharding import PartitionSpec as P

EPS = 1e-06
CHUNKS = 4
TILE = 256
VMEM_BYTES = 67000000


def slot_index(route_ids, experts, capacity):
    rows, top = route_ids.shape
    hit = [route_ids[:, k : k + 1] == jnp.arange(experts, dtype=jnp.int32)[None, :] for k in range(top)]
    named = sum(h.astype(jnp.float32) for h in hit)
    before = (jnp.arange(rows)[:, None] > jnp.arange(rows)[None, :]).astype(jnp.bfloat16)
    ranked = jnp.dot(before, named.astype(jnp.bfloat16), preferred_element_type=jnp.float32)
    base = ranked + jnp.arange(experts, dtype=jnp.float32)[None, :] * capacity
    return jnp.stack([jnp.sum(jnp.where(h, base, 0.0), axis=1) for h in hit])


def dot32(a, b):
    return jnp.dot(a, b, preferred_element_type=jnp.float32)


HOME, ACROSS, BEYOND, NEAR = range(4)


def kernel(
    devices, capacity, top,
    tokens_hbm, gain, table, gate_hbm, up_hbm, down_hbm,
    mixed,
    normed, far, tables, takes, gives, take_near, give_near, packed, packed_near, arrived, hidden,
    w_gate, w_up, w_down, backs, backs_near, partial_in,
    load_sems, table_send, table_recv, far_send, far_recv, go_send, go_recv, back_send, back_recv,
    relay_send, relay_recv, part_send, part_recv,
):
    m = devices // 4
    half = 2 * m
    unit = m * capacity
    chunks, rows, step = normed.shape
    ff = w_gate.shape[1]
    me = lax.axis_index("ep")
    side = me // half
    plane = me // m
    j = me % m
    q = me % half
    own = plane * m
    hub = (1 + side) * m
    leaf = 3 * side * m
    other_hub = (2 - side) * m + j
    is_hub = plane * (3 - plane) > 0

    barrier = pltpu.get_barrier_semaphore()

    def greet(i, carry):
        pl.semaphore_signal(barrier, inc=1, device_id={"ep": side * half + (q + 1 + i) % half})
        return carry

    token_load = pltpu.make_async_copy(tokens_hbm, mixed, load_sems.at[3])
    token_load.start()
    lax.fori_loop(0, half - 1, greet, 0)

    @pl.when(is_hub)
    def _():
        pl.semaphore_signal(barrier, inc=1, device_id={"ep": other_hub})

    loads = [
        pltpu.make_async_copy(gate_hbm.at[0], w_gate, load_sems.at[0]),
        pltpu.make_async_copy(up_hbm.at[0], w_up, load_sems.at[1]),
        pltpu.make_async_copy(down_hbm.at[0], w_down, load_sems.at[2]),
    ]
    token_load.wait()

    def norm(i, carry):
        at = pl.ds(pl.multiple_of(i * 64, 64), 64)
        floats = mixed[at, :].astype(jnp.float32)
        scale = lax.rsqrt(jnp.mean(floats * floats, axis=-1, keepdims=True) + EPS)
        value = (floats * scale * gain[...]).astype(jnp.bfloat16)
        for c in range(chunks):
            normed[c, at, :] = value[:, c * step : (c + 1) * step]
        return carry

    lax.fori_loop(0, rows // 64, norm, 0)

    @pl.when(is_hub)
    def _():
        pl.semaphore_wait(barrier, half)

    @pl.when(jnp.logical_not(is_hub))
    def _():
        pl.semaphore_wait(barrier, half - 1)

    def remote(src, dst, send, recv, device):
        return pltpu.make_async_remote_copy(
            src_ref=src, dst_ref=dst, send_sem=send, recv_sem=recv, device_id={"ep": device}
        )

    def table_copy(r, src, device):
        return remote(src, tables.at[r - 1], table_send.at[r - 1], table_recv.at[r - 1], device)

    def far_copy(r, c, src, device):
        return remote(src.at[c], far.at[r - 1, c], far_send.at[r - 1, c], far_recv.at[r - 1, c], device)

    def part_copy(k, c, src, slot, device):
        return remote(src.at[c], partial_in.at[slot, c], part_send.at[k, c], part_recv.at[slot, c], device)

    def span(i, part=0):
        return pl.ds(pl.multiple_of(part * unit + i * capacity, 16), capacity)

    def packs(r, c):
        return packed_near.at[c] if r == NEAR else packed.at[r, c]

    def returns(r, c):
        return backs_near.at[c] if r == NEAR else backs.at[r, c]

    def go_copy(r, c, part, i):
        target = (leaf if part else own) + i
        return remote(
            packs(r, c).at[span(i, part)], arrived.at[r, c, span(j)],
            go_send.at[r, c, part * m + i], go_recv.at[r, c, j], target,
        )

    def go_arrival(r, c, i, base):
        return remote(
            arrived.at[r, c, span(i)], arrived.at[r, c, span(i)],
            go_send.at[r, c, 0], go_recv.at[r, c, i], base + i,
        )

    def back_copy(r, c, i):
        return remote(
            arrived.at[r, c, span(i)], returns(r, c).at[span(j)],
            back_send.at[r, c, i], back_recv.at[r, c, j], own + i,
        )

    def back_arrival(r, c, i):
        return remote(
            arrived.at[r, c, span(i)], returns(r, c).at[span(i)],
            back_send.at[r, c, 0], back_recv.at[r, c, i], own + i,
        )

    def relay_copy(r, c):
        return remote(
            backs.at[r, c, pl.ds(0, unit)], backs.at[r, c, pl.ds(unit, unit)],
            relay_send.at[r, c], relay_recv.at[r, c], hub + j,
        )

    def others(act):
        def one(i, carry):
            act((j + 1 + i) % m)
            return carry

        lax.fori_loop(0, m - 1, one, 0)

    def everyone(act):
        def one(i, carry):
            act((j + i) % m)
            return carry

        lax.fori_loop(0, m, one, 0)

    def matrices(source, take, give, bases):
        width = 128

        def block(part, first):
            def one(i, carry):
                at = pl.multiple_of(part * unit + i * width, width)
                start = first * capacity + i * width
                slots = (start + lax.broadcasted_iota(jnp.int32, (width, rows), 0)).astype(jnp.float32)
                taken = jnp.zeros((width, rows), jnp.float32)
                total = jnp.zeros((width, rows), jnp.float32)
                for k in range(top):
                    hit = source[k : k + 1, :] == slots
                    taken = taken + jnp.where(hit, 1.0, 0.0)
                    total = total + jnp.where(hit, source[top + k : top + k + 1, :], 0.0)
                take[pl.ds(at, width), :] = taken.astype(jnp.bfloat16)
                give[:, pl.ds(at, width)] = total.T.astype(jnp.bfloat16)
                return carry

            lax.fori_loop(0, unit // width, one, 0)

        for part, first in enumerate(bases):
            block(part, first)

    def tiles(act):
        def one(i, carry):
            act(pl.ds(pl.multiple_of(i * TILE, TILE), TILE))
            return carry

        lax.fori_loop(0, step // TILE, one, 0)

    def pack(r, c, source):
        take = take_near if r == NEAR else takes.at[r]
        target = packs(r, c)

        def one(cols):
            target[:, cols] = dot32(take[...], source[c, :, cols]).astype(jnp.bfloat16)

        tiles(one)
        if r != NEAR:
            everyone(lambda i: go_copy(r, c, 1, i).start())
        others(lambda i: go_copy(r, c, 0, i).start())
        arrived[r, c, span(j), :] = target[span(j), :]

    def expert(r):
        def gated(i, carry):
            cols = pl.ds(pl.multiple_of(i * TILE, TILE), TILE)
            gate_pre = dot32(arrived[r, 0], w_gate[0:step, cols])
            up_pre = dot32(arrived[r, 0], w_up[0:step, cols])
            for c in range(1, chunks):
                gate_pre += dot32(arrived[r, c], w_gate[c * step : (c + 1) * step, cols])
                up_pre += dot32(arrived[r, c], w_up[c * step : (c + 1) * step, cols])
            hidden[:, cols] = (gate_pre / (1.0 + jnp.exp(-gate_pre)) * up_pre).astype(jnp.bfloat16)
            return carry

        lax.fori_loop(0, ff // TILE, gated, 0)
        for c in range(chunks):

            def out(i, carry):
                at = pl.multiple_of(i * TILE, TILE)
                cols = pl.ds(pl.multiple_of(c * step + at, TILE), TILE)
                arrived[r, c, :, pl.ds(at, TILE)] = dot32(hidden[...], w_down[:, cols]).astype(jnp.bfloat16)
                return carry

            lax.fori_loop(0, step // TILE, out, 0)
            others(lambda i: back_copy(r, c, i).start())
            returns(r, c)[span(j), :] = arrived[r, c, span(j), :]

    def wait_back(r, c):
        others(lambda i: back_arrival(r, c, i).wait_recv())

    def hub_role():
        bases = (hub, leaf)
        far_copy(ACROSS, 0, normed, other_hub).start()
        table_copy(ACROSS, table, other_hub).start()
        for load in loads:
            load.start()
        matrices(table, takes.at[HOME], gives.at[HOME], bases)
        table_copy(NEAR, table, leaf + j).wait_recv()
        table_copy(BEYOND, tables.at[NEAR - 1], other_hub).start()
        for c in range(chunks):
            pack(HOME, c, normed)
        matrices(tables.at[NEAR - 1], take_near, give_near, (own,))

        def near_in(c):
            far_copy(NEAR, c, normed, leaf + j).wait_recv()
            far_copy(BEYOND, c, far.at[NEAR - 1], other_hub).start()
            pack(NEAR, c, far.at[NEAR - 1])

        def far_in(r, c):
            far_copy(r, c, normed, other_hub).wait_recv()
            pack(r, c, far.at[r - 1])

        def settle(r):
            for c in range(chunks):
                others(lambda i: go_arrival(r, c, i, own).wait_recv())

        def merge(r, c):
            wait_back(r, c)
            relay_copy(r, c).wait_recv()

            def one(cols):
                far[r - 1, c, :, cols] = dot32(gives[r], backs[r, c, :, cols]).astype(jnp.bfloat16)

            tiles(one)
            slot = 0 if r == ACROSS else 1
            part_copy(slot, c, far.at[r - 1], slot, other_hub).start()

        def pass_on(c):
            wait_back(NEAR, c)
            part_copy(1, c, normed, 1, other_hub).wait_recv()
            far_copy(BEYOND, c, far.at[NEAR - 1], other_hub).wait_send()

            def one(cols):
                total = dot32(give_near[...], backs_near[c, :, cols]) + partial_in[1, c, :, cols].astype(jnp.float32)
                far[NEAR - 1, c, :, cols] = total.astype(jnp.bfloat16)

            tiles(one)
            part_copy(2, c, far.at[NEAR - 1], 1, leaf + j).start()

        near_in(0)
        table_copy(ACROSS, table, other_hub).wait_recv()
        matrices(tables.at[ACROSS - 1], takes.at[ACROSS], gives.at[ACROSS], bases)
        far_in(ACROSS, 0)
        table_copy(BEYOND, table, other_hub).wait_recv()
        matrices(tables.at[BEYOND - 1], takes.at[BEYOND], gives.at[BEYOND], bases)
        near_in(1)
        far_in(BEYOND, 0)
        near_in(2)
        far_in(BEYOND, 1)
        near_in(3)
        for c in range(1, chunks):
            far_copy(ACROSS, c, normed, other_hub).start()
        far_in(BEYOND, 2)
        for load in loads:
            load.wait()
        settle(HOME)
        expert(HOME)
        far_in(BEYOND, 3)
        settle(NEAR)
        expert(NEAR)
        settle(BEYOND)
        expert(BEYOND)
        far_in(ACROSS, 1)
        far_in(ACROSS, 2)
        merge(BEYOND, 0)
        far_in(ACROSS, 3)
        settle(ACROSS)
        expert(ACROSS)
        merge(BEYOND, 1)
        merge(BEYOND, 2)
        pass_on(0)
        merge(BEYOND, 3)
        pass_on(1)
        merge(ACROSS, 0)
        pass_on(2)
        merge(ACROSS, 1)
        merge(ACROSS, 2)
        pass_on(3)
        merge(ACROSS, 3)
        for c in range(chunks):
            wait_back(HOME, c)
            relay_copy(HOME, c).wait_recv()
            part_copy(0, c, normed, 0, other_hub).wait_recv()

            def close(i, carry):
                at = pl.multiple_of(i * TILE, TILE)
                cols = pl.ds(at, TILE)
                total = dot32(gives[HOME], backs[HOME, c, :, cols]) + partial_in[0, c, :, cols].astype(jnp.float32)
                mixed[:, pl.ds(pl.multiple_of(c * step + at, TILE), TILE)] = total.astype(jnp.bfloat16)
                return carry

            lax.fori_loop(0, step // TILE, close, 0)
        table_copy(ACROSS, table, other_hub).wait_send()
        table_copy(BEYOND, table, other_hub).wait_send()
        for c in range(chunks):
            far_copy(ACROSS, c, normed, other_hub).wait_send()
            for k in range(3):
                part_copy(k, c, normed, 0, other_hub).wait_send()
            for r in (HOME, ACROSS, BEYOND):
                everyone(lambda i: go_copy(r, c, 1, i).wait_send())

    def leaf_role():
        table_copy(NEAR, table, hub + j).start()
        for c in range(chunks):
            far_copy(NEAR, c, normed, hub + j).start()
        for load in loads:
            load.start()
        matrices(table, take_near, give_near, (own,))
        for c in range(chunks):
            pack(NEAR, c, normed)
        for load in loads:
            load.wait()
        for c in range(chunks):
            others(lambda i: go_arrival(NEAR, c, i, own).wait_recv())
        expert(NEAR)
        for r in (HOME, BEYOND, ACROSS):
            for c in range(chunks):
                everyone(lambda i: go_arrival(r, c, i, hub).wait_recv())
            expert(r)
            for c in range(chunks):
                wait_back(r, c)
                relay_copy(r, c).start()
        for c in range(chunks):
            wait_back(NEAR, c)
            part_copy(2, c, normed, 1, hub + j).wait_recv()

            def close(i, carry):
                at = pl.multiple_of(i * TILE, TILE)
                cols = pl.ds(at, TILE)
                total = dot32(give_near[...], backs_near[c, :, cols]) + partial_in[1, c, :, cols].astype(jnp.float32)
                mixed[:, pl.ds(pl.multiple_of(c * step + at, TILE), TILE)] = total.astype(jnp.bfloat16)
                return carry

            lax.fori_loop(0, step // TILE, close, 0)
        table_copy(NEAR, table, hub + j).wait_send()
        for c in range(chunks):
            far_copy(NEAR, c, normed, hub + j).wait_send()
            for r in (HOME, ACROSS, BEYOND):
                relay_copy(r, c).wait_send()

    @pl.when(is_hub)
    def _():
        hub_role()

    @pl.when(jnp.logical_not(is_hub))
    def _():
        leaf_role()

    def drain(r):
        for c in range(chunks):
            others(lambda i: back_copy(r, c, i).wait_send())

    for r in range(4):
        drain(r)
    for c in range(chunks):
        others(lambda i: go_copy(NEAR, c, 0, i).wait_send())

    @pl.when(is_hub)
    def _():
        for r in (HOME, ACROSS, BEYOND):
            for c in range(chunks):
                others(lambda i: go_copy(r, c, 0, i).wait_send())


def body(tokens, norm_gain, route_ids, route_gates, w_gate, w_up, w_down):
    rows, width = tokens.shape
    top = route_ids.shape[1]
    devices = lax.axis_size("ep")
    experts = devices
    ff = w_gate.shape[2]
    capacity = 3 * rows * top // (2 * experts)
    m = devices // 4
    unit = m * capacity
    step = width // CHUNKS
    weights = (route_gates / jnp.sum(route_gates, axis=1, keepdims=True)).T
    table = jnp.concatenate([slot_index(route_ids, experts, capacity), weights])
    vmem = pl.BlockSpec(memory_space=pltpu.VMEM)
    hbm = pl.BlockSpec(memory_space=pl.ANY)
    bf16 = jnp.bfloat16
    dma = pltpu.SemaphoreType.DMA
    return pl.pallas_call(
        functools.partial(kernel, devices, capacity, top),
        out_shape=jax.ShapeDtypeStruct((rows, width), bf16),
        in_specs=[hbm, vmem, vmem, hbm, hbm, hbm],
        out_specs=vmem,
        scratch_shapes=[
            pltpu.VMEM((CHUNKS, rows, step), bf16),
            pltpu.VMEM((3, CHUNKS, rows, step), bf16),
            pltpu.VMEM((3, *table.shape), jnp.float32),
            pltpu.VMEM((3, 2 * unit, rows), bf16),
            pltpu.VMEM((3, rows, 2 * unit), bf16),
            pltpu.VMEM((unit, rows), bf16),
            pltpu.VMEM((rows, unit), bf16),
            pltpu.VMEM((3, CHUNKS, 2 * unit, step), bf16),
            pltpu.VMEM((CHUNKS, unit, step), bf16),
            pltpu.VMEM((4, CHUNKS, unit, step), bf16),
            pltpu.VMEM((unit, ff), bf16),
            pltpu.VMEM((width, ff), bf16),
            pltpu.VMEM((width, ff), bf16),
            pltpu.VMEM((ff, width), bf16),
            pltpu.VMEM((3, CHUNKS, 2 * unit, step), bf16),
            pltpu.VMEM((CHUNKS, unit, step), bf16),
            pltpu.VMEM((2, CHUNKS, rows, step), bf16),
            dma((4,)),
            dma((3,)),
            dma((3,)),
            dma((3, CHUNKS)),
            dma((3, CHUNKS)),
            dma((4, CHUNKS, 2 * m)),
            dma((4, CHUNKS, m)),
            dma((4, CHUNKS, m)),
            dma((4, CHUNKS, m)),
            dma((3, CHUNKS)),
            dma((3, CHUNKS)),
            dma((3, CHUNKS)),
            dma((2, CHUNKS)),
        ],
        compiler_params=pltpu.CompilerParams(
            collective_id=0, has_side_effects=True, vmem_limit_bytes=VMEM_BYTES
        ),
    )(tokens, norm_gain[None, :], table, w_gate, w_up, w_down)


def solution(mesh):
    placed = (
        P(("grp", "ep"), None),
        P(),
        P(("grp", "ep"), None),
        P(("grp", "ep"), None),
        P("ep", None, None),
        P("ep", None, None),
        P("ep", None, None),
    )
    return jax.shard_map(
        body, mesh=mesh, in_specs=placed, out_specs=P(("grp", "ep"), None), check_vma=False
    )
```

```python
import functools

import jax
import jax.numpy as jnp
from jax import lax
from jax.experimental import pallas as pl
from jax.experimental.pallas import tpu as pltpu
from jax.sharding import PartitionSpec as P

EPS = 1e-06
CHUNKS = 4
TILE = 256
VMEM_BYTES = 67000000


def slot_index(route_ids, experts, capacity):
    rows, top = route_ids.shape
    hit = [route_ids[:, k : k + 1] == jnp.arange(experts, dtype=jnp.int32)[None, :] for k in range(top)]
    named = sum(h.astype(jnp.float32) for h in hit)
    before = (jnp.arange(rows)[:, None] > jnp.arange(rows)[None, :]).astype(jnp.bfloat16)
    ranked = jnp.dot(before, named.astype(jnp.bfloat16), preferred_element_type=jnp.float32)
    base = ranked + jnp.arange(experts, dtype=jnp.float32)[None, :] * capacity
    return jnp.stack([jnp.sum(jnp.where(h, base, 0.0), axis=1) for h in hit])


def dot32(a, b):
    return jnp.dot(a, b, preferred_element_type=jnp.float32)


HOME, ACROSS, BEYOND, NEAR = range(4)


def kernel(
    devices, capacity, top,
    tokens_hbm, gain, table, gate_hbm, up_hbm, down_hbm,
    mixed,
    normed, far, tables, takes, gives, take_near, give_near, packed, packed_near, arrived, hidden,
    w_gate, w_up, w_down, backs, backs_near, partial_in,
    load_sems, table_send, table_recv, far_send, far_recv, go_send, go_recv, back_send, back_recv,
    relay_send, relay_recv, part_send, part_recv,
):
    m = devices // 4
    half = 2 * m
    unit = m * capacity
    chunks, rows, step = normed.shape
    ff = w_gate.shape[1]
    me = lax.axis_index("ep")
    side = me // half
    plane = me // m
    j = me % m
    q = me % half
    own = plane * m
    hub = (1 + side) * m
    leaf = 3 * side * m
    other_hub = (2 - side) * m + j
    is_hub = plane * (3 - plane) > 0

    barrier = pltpu.get_barrier_semaphore()

    def greet(i, carry):
        pl.semaphore_signal(barrier, inc=1, device_id={"ep": side * half + (q + 1 + i) % half})
        return carry

    token_load = pltpu.make_async_copy(tokens_hbm, mixed, load_sems.at[3])
    token_load.start()
    lax.fori_loop(0, half - 1, greet, 0)

    @pl.when(is_hub)
    def _():
        pl.semaphore_signal(barrier, inc=1, device_id={"ep": other_hub})

    loads = [
        pltpu.make_async_copy(gate_hbm.at[0], w_gate, load_sems.at[0]),
        pltpu.make_async_copy(up_hbm.at[0], w_up, load_sems.at[1]),
        pltpu.make_async_copy(down_hbm.at[0], w_down, load_sems.at[2]),
    ]
    token_load.wait()

    def norm(i, carry):
        at = pl.ds(pl.multiple_of(i * 64, 64), 64)
        floats = mixed[at, :].astype(jnp.float32)
        scale = lax.rsqrt(jnp.mean(floats * floats, axis=-1, keepdims=True) + EPS)
        value = (floats * scale * gain[...]).astype(jnp.bfloat16)
        for c in range(chunks):
            normed[c, at, :] = value[:, c * step : (c + 1) * step]
        return carry

    lax.fori_loop(0, rows // 64, norm, 0)

    @pl.when(is_hub)
    def _():
        pl.semaphore_wait(barrier, half)

    @pl.when(jnp.logical_not(is_hub))
    def _():
        pl.semaphore_wait(barrier, half - 1)

    def remote(src, dst, send, recv, device):
        return pltpu.make_async_remote_copy(
            src_ref=src, dst_ref=dst, send_sem=send, recv_sem=recv, device_id={"ep": device}
        )

    def table_copy(r, src, device):
        return remote(src, tables.at[r - 1], table_send.at[r - 1], table_recv.at[r - 1], device)

    def far_copy(r, c, src, device):
        return remote(src.at[c], far.at[r - 1, c], far_send.at[r - 1, c], far_recv.at[r - 1, c], device)

    def part_copy(k, c, src, slot, device):
        return remote(src.at[c], partial_in.at[slot, c], part_send.at[k, c], part_recv.at[slot, c], device)

    def span(i, part=0):
        return pl.ds(pl.multiple_of(part * unit + i * capacity, 16), capacity)

    def packs(r, c):
        return packed_near.at[c] if r == NEAR else packed.at[r, c]

    def returns(r, c):
        return backs_near.at[c] if r == NEAR else backs.at[r, c]

    def go_copy(r, c, part, i):
        target = (leaf if part else own) + i
        return remote(
            packs(r, c).at[span(i, part)], arrived.at[r, c, span(j)],
            go_send.at[r, c, part * m + i], go_recv.at[r, c, j], target,
        )

    def go_arrival(r, c, i, base):
        return remote(
            arrived.at[r, c, span(i)], arrived.at[r, c, span(i)],
            go_send.at[r, c, 0], go_recv.at[r, c, i], base + i,
        )

    def back_copy(r, c, i):
        return remote(
            arrived.at[r, c, span(i)], returns(r, c).at[span(j)],
            back_send.at[r, c, i], back_recv.at[r, c, j], own + i,
        )

    def back_arrival(r, c, i):
        return remote(
            arrived.at[r, c, span(i)], returns(r, c).at[span(i)],
            back_send.at[r, c, 0], back_recv.at[r, c, i], own + i,
        )

    def relay_copy(r, c):
        return remote(
            backs.at[r, c, pl.ds(0, unit)], backs.at[r, c, pl.ds(unit, unit)],
            relay_send.at[r, c], relay_recv.at[r, c], hub + j,
        )

    def others(act):
        def one(i, carry):
            act((j + 1 + i) % m)
            return carry

        lax.fori_loop(0, m - 1, one, 0)

    def everyone(act):
        def one(i, carry):
            act((j + i) % m)
            return carry

        lax.fori_loop(0, m, one, 0)

    def matrices(source, take, give, bases):
        width = 128

        def block(part, first):
            def one(i, carry):
                at = pl.multiple_of(part * unit + i * width, width)
                start = first * capacity + i * width
                slots = (start + lax.broadcasted_iota(jnp.int32, (width, rows), 0)).astype(jnp.float32)
                taken = jnp.zeros((width, rows), jnp.float32)
                total = jnp.zeros((width, rows), jnp.float32)
                for k in range(top):
                    hit = source[k : k + 1, :] == slots
                    taken = taken + jnp.where(hit, 1.0, 0.0)
                    total = total + jnp.where(hit, source[top + k : top + k + 1, :], 0.0)
                take[pl.ds(at, width), :] = taken.astype(jnp.bfloat16)
                give[:, pl.ds(at, width)] = total.T.astype(jnp.bfloat16)
                return carry

            lax.fori_loop(0, unit // width, one, 0)

        for part, first in enumerate(bases):
            block(part, first)

    def tiles(act):
        def one(i, carry):
            act(pl.ds(pl.multiple_of(i * TILE, TILE), TILE))
            return carry

        lax.fori_loop(0, step // TILE, one, 0)

    def pack(r, c, source):
        take = take_near if r == NEAR else takes.at[r]
        target = packs(r, c)

        def one(cols):
            target[:, cols] = dot32(take[...], source[c, :, cols]).astype(jnp.bfloat16)

        tiles(one)
        if r != NEAR:
            everyone(lambda i: go_copy(r, c, 1, i).start())
        others(lambda i: go_copy(r, c, 0, i).start())
        arrived[r, c, span(j), :] = target[span(j), :]

    def hand_back(r, c):
        others(lambda i: back_copy(r, c, i).start())
        returns(r, c)[span(j), :] = arrived[r, c, span(j), :]

    def expert(r, send):
        def gated(i, carry):
            cols = pl.ds(pl.multiple_of(i * TILE, TILE), TILE)
            gate_pre = dot32(arrived[r, 0], w_gate[0:step, cols])
            up_pre = dot32(arrived[r, 0], w_up[0:step, cols])
            for c in range(1, chunks):
                gate_pre += dot32(arrived[r, c], w_gate[c * step : (c + 1) * step, cols])
                up_pre += dot32(arrived[r, c], w_up[c * step : (c + 1) * step, cols])
            hidden[:, cols] = (gate_pre / (1.0 + jnp.exp(-gate_pre)) * up_pre).astype(jnp.bfloat16)
            return carry

        lax.fori_loop(0, ff // TILE, gated, 0)
        for c in range(chunks):

            def out(i, carry):
                at = pl.multiple_of(i * TILE, TILE)
                cols = pl.ds(pl.multiple_of(c * step + at, TILE), TILE)
                arrived[r, c, :, pl.ds(at, TILE)] = dot32(hidden[...], w_down[:, cols]).astype(jnp.bfloat16)
                return carry

            lax.fori_loop(0, step // TILE, out, 0)
            if send:
                hand_back(r, c)

    def wait_back(r, c):
        others(lambda i: back_arrival(r, c, i).wait_recv())

    def hub_role():
        bases = (hub, leaf)
        far_copy(ACROSS, 0, normed, other_hub).start()
        table_copy(ACROSS, table, other_hub).start()
        for load in loads:
            load.start()
        matrices(table, takes.at[HOME], gives.at[HOME], bases)
        table_copy(NEAR, table, leaf + j).wait_recv()
        table_copy(BEYOND, tables.at[NEAR - 1], other_hub).start()
        for c in range(chunks):
            pack(HOME, c, normed)
        matrices(tables.at[NEAR - 1], take_near, give_near, (own,))

        def near_in(c):
            far_copy(NEAR, c, normed, leaf + j).wait_recv()
            far_copy(BEYOND, c, far.at[NEAR - 1], other_hub).start()
            pack(NEAR, c, far.at[NEAR - 1])

        def far_in(r, c):
            far_copy(r, c, normed, other_hub).wait_recv()
            pack(r, c, far.at[r - 1])

        def settle(r):
            for c in range(chunks):
                others(lambda i: go_arrival(r, c, i, own).wait_recv())

        def merge(r, c):
            wait_back(r, c)
            relay_copy(r, c).wait_recv()

            def one(cols):
                far[r - 1, c, :, cols] = dot32(gives[r], backs[r, c, :, cols]).astype(jnp.bfloat16)

            tiles(one)
            slot = 0 if r == ACROSS else 1
            part_copy(slot, c, far.at[r - 1], slot, other_hub).start()

        def pass_on(c):
            wait_back(NEAR, c)
            part_copy(1, c, normed, 1, other_hub).wait_recv()
            far_copy(BEYOND, c, far.at[NEAR - 1], other_hub).wait_send()

            def one(cols):
                total = dot32(give_near[...], backs_near[c, :, cols]) + partial_in[1, c, :, cols].astype(jnp.float32)
                far[NEAR - 1, c, :, cols] = total.astype(jnp.bfloat16)

            tiles(one)
            part_copy(2, c, far.at[NEAR - 1], 1, leaf + j).start()

        near_in(0)
        table_copy(ACROSS, table, other_hub).wait_recv()
        matrices(tables.at[ACROSS - 1], takes.at[ACROSS], gives.at[ACROSS], bases)
        table_copy(BEYOND, table, other_hub).wait_recv()
        matrices(tables.at[BEYOND - 1], takes.at[BEYOND], gives.at[BEYOND], bases)
        near_in(1)
        far_in(BEYOND, 0)
        near_in(2)
        far_in(BEYOND, 1)
        near_in(3)
        for c in range(1, chunks):
            far_copy(ACROSS, c, normed, other_hub).start()
        far_in(BEYOND, 2)
        for load in loads:
            load.wait()
        settle(HOME)
        expert(HOME, False)
        far_in(BEYOND, 3)
        settle(BEYOND)
        expert(BEYOND, True)
        far_in(ACROSS, 0)
        far_in(ACROSS, 1)
        settle(NEAR)
        expert(NEAR, False)
        far_in(ACROSS, 2)
        hand_back(NEAR, 0)
        hand_back(NEAR, 1)
        far_in(ACROSS, 3)
        merge(BEYOND, 0)
        hand_back(NEAR, 2)
        hand_back(NEAR, 3)
        merge(BEYOND, 1)
        settle(ACROSS)
        expert(ACROSS, True)
        merge(BEYOND, 2)
        pass_on(0)
        merge(BEYOND, 3)
        pass_on(1)
        for c in range(chunks):
            hand_back(HOME, c)
        merge(ACROSS, 0)
        pass_on(2)
        merge(ACROSS, 1)
        merge(ACROSS, 2)
        pass_on(3)
        merge(ACROSS, 3)
        for c in range(chunks):
            wait_back(HOME, c)
            relay_copy(HOME, c).wait_recv()
            part_copy(0, c, normed, 0, other_hub).wait_recv()

            def close(i, carry):
                at = pl.multiple_of(i * TILE, TILE)
                cols = pl.ds(at, TILE)
                total = dot32(gives[HOME], backs[HOME, c, :, cols]) + partial_in[0, c, :, cols].astype(jnp.float32)
                mixed[:, pl.ds(pl.multiple_of(c * step + at, TILE), TILE)] = total.astype(jnp.bfloat16)
                return carry

            lax.fori_loop(0, step // TILE, close, 0)
        table_copy(ACROSS, table, other_hub).wait_send()
        table_copy(BEYOND, table, other_hub).wait_send()
        for c in range(chunks):
            far_copy(ACROSS, c, normed, other_hub).wait_send()
            for k in range(3):
                part_copy(k, c, normed, 0, other_hub).wait_send()
            for r in (HOME, ACROSS, BEYOND):
                everyone(lambda i: go_copy(r, c, 1, i).wait_send())

    def leaf_role():
        table_copy(NEAR, table, hub + j).start()
        for c in range(chunks):
            far_copy(NEAR, c, normed, hub + j).start()
        for load in loads:
            load.start()
        matrices(table, take_near, give_near, (own,))
        for load in loads:
            load.wait()

        def settle(r):
            for c in range(chunks):
                everyone(lambda i: go_arrival(r, c, i, hub).wait_recv())

        def send_on(r, c):
            wait_back(r, c)
            relay_copy(r, c).start()

        settle(HOME)
        expert(HOME, True)
        for c in range(chunks - 1):
            send_on(HOME, c)
        settle(BEYOND)
        expert(BEYOND, True)
        send_on(HOME, chunks - 1)
        for c in range(chunks):
            send_on(BEYOND, c)
        settle(ACROSS)
        expert(ACROSS, True)
        for c in range(chunks):
            pack(NEAR, c, normed)
        for c in range(chunks):
            send_on(ACROSS, c)
        for c in range(chunks):
            others(lambda i: go_arrival(NEAR, c, i, own).wait_recv())
        expert(NEAR, True)
        for c in range(chunks):
            wait_back(NEAR, c)
            part_copy(2, c, normed, 1, hub + j).wait_recv()

            def close(i, carry):
                at = pl.multiple_of(i * TILE, TILE)
                cols = pl.ds(at, TILE)
                total = dot32(give_near[...], backs_near[c, :, cols]) + partial_in[1, c, :, cols].astype(jnp.float32)
                mixed[:, pl.ds(pl.multiple_of(c * step + at, TILE), TILE)] = total.astype(jnp.bfloat16)
                return carry

            lax.fori_loop(0, step // TILE, close, 0)
        table_copy(NEAR, table, hub + j).wait_send()
        for c in range(chunks):
            far_copy(NEAR, c, normed, hub + j).wait_send()
            for r in (HOME, ACROSS, BEYOND):
                relay_copy(r, c).wait_send()

    @pl.when(is_hub)
    def _():
        hub_role()

    @pl.when(jnp.logical_not(is_hub))
    def _():
        leaf_role()

    def drain(r):
        for c in range(chunks):
            others(lambda i: back_copy(r, c, i).wait_send())

    for r in range(4):
        drain(r)
    for c in range(chunks):
        others(lambda i: go_copy(NEAR, c, 0, i).wait_send())

    @pl.when(is_hub)
    def _():
        for r in (HOME, ACROSS, BEYOND):
            for c in range(chunks):
                others(lambda i: go_copy(r, c, 0, i).wait_send())


def body(tokens, norm_gain, route_ids, route_gates, w_gate, w_up, w_down):
    rows, width = tokens.shape
    top = route_ids.shape[1]
    devices = lax.axis_size("ep")
    experts = devices
    ff = w_gate.shape[2]
    capacity = 3 * rows * top // (2 * experts)
    m = devices // 4
    unit = m * capacity
    step = width // CHUNKS
    weights = (route_gates / jnp.sum(route_gates, axis=1, keepdims=True)).T
    table = jnp.concatenate([slot_index(route_ids, experts, capacity), weights])
    vmem = pl.BlockSpec(memory_space=pltpu.VMEM)
    hbm = pl.BlockSpec(memory_space=pl.ANY)
    bf16 = jnp.bfloat16
    dma = pltpu.SemaphoreType.DMA
    return pl.pallas_call(
        functools.partial(kernel, devices, capacity, top),
        out_shape=jax.ShapeDtypeStruct((rows, width), bf16),
        in_specs=[hbm, vmem, vmem, hbm, hbm, hbm],
        out_specs=vmem,
        scratch_shapes=[
            pltpu.VMEM((CHUNKS, rows, step), bf16),
            pltpu.VMEM((3, CHUNKS, rows, step), bf16),
            pltpu.VMEM((3, *table.shape), jnp.float32),
            pltpu.VMEM((3, 2 * unit, rows), bf16),
            pltpu.VMEM((3, rows, 2 * unit), bf16),
            pltpu.VMEM((unit, rows), bf16),
            pltpu.VMEM((rows, unit), bf16),
            pltpu.VMEM((3, CHUNKS, 2 * unit, step), bf16),
            pltpu.VMEM((CHUNKS, unit, step), bf16),
            pltpu.VMEM((4, CHUNKS, unit, step), bf16),
            pltpu.VMEM((unit, ff), bf16),
            pltpu.VMEM((width, ff), bf16),
            pltpu.VMEM((width, ff), bf16),
            pltpu.VMEM((ff, width), bf16),
            pltpu.VMEM((3, CHUNKS, 2 * unit, step), bf16),
            pltpu.VMEM((CHUNKS, unit, step), bf16),
            pltpu.VMEM((2, CHUNKS, rows, step), bf16),
            dma((4,)),
            dma((3,)),
            dma((3,)),
            dma((3, CHUNKS)),
            dma((3, CHUNKS)),
            dma((4, CHUNKS, 2 * m)),
            dma((4, CHUNKS, m)),
            dma((4, CHUNKS, m)),
            dma((4, CHUNKS, m)),
            dma((3, CHUNKS)),
            dma((3, CHUNKS)),
            dma((3, CHUNKS)),
            dma((2, CHUNKS)),
        ],
        compiler_params=pltpu.CompilerParams(
            collective_id=0, has_side_effects=True, vmem_limit_bytes=VMEM_BYTES
        ),
    )(tokens, norm_gain[None, :], table, w_gate, w_up, w_down)


def solution(mesh):
    placed = (
        P(("grp", "ep"), None),
        P(),
        P(("grp", "ep"), None),
        P(("grp", "ep"), None),
        P("ep", None, None),
        P("ep", None, None),
        P("ep", None, None),
    )
    return jax.shard_map(
        body, mesh=mesh, in_specs=placed, out_specs=P(("grp", "ep"), None), check_vma=False
    )
```

```python
import functools

import jax
import jax.numpy as jnp
from jax import lax
from jax.experimental import pallas as pl
from jax.experimental.pallas import tpu as pltpu
from jax.sharding import PartitionSpec as P

EPS = 1e-06
CHUNKS = 8
TILE = 256
VMEM_BYTES = 67000000


def dot32(a, b):
    return jnp.dot(a, b, preferred_element_type=jnp.float32)


HOME, ACROSS, BEYOND, NEAR = range(4)


def kernel(
    devices, capacity, top,
    tokens_hbm, gain, route_ids, route_gates, gate_hbm, up_hbm, down_hbm,
    mixed_hbm,
    mixed, table, normed, far, tables, takes, gives, take_near, give_near, packed, packed_near, arrived, hidden,
    w_gate, w_up, w_down, backs, backs_near, partial_in,
    load_sems, table_send, table_recv, far_send, far_recv, go_send, go_recv, back_send, back_recv,
    relay_send, relay_recv, part_send, part_recv, out_sem,
):
    m = devices // 4
    half = 2 * m
    unit = m * capacity
    chunks, rows, step = normed.shape
    ff = w_gate.shape[1]
    me = lax.axis_index("ep")
    side = me // half
    plane = me // m
    j = me % m
    q = me % half
    own = plane * m
    hub = (1 + side) * m
    leaf = 3 * side * m
    other_hub = (2 - side) * m + j
    peer = own + (j + 1) % m
    is_hub = plane * (3 - plane) > 0

    barrier = pltpu.get_barrier_semaphore()

    def greet(i, carry):
        pl.semaphore_signal(barrier, inc=1, device_id={"ep": side * half + (q + 1 + i) % half})
        return carry

    token_load = pltpu.make_async_copy(tokens_hbm, mixed, load_sems.at[3])
    token_load.start()
    lax.fori_loop(0, half - 1, greet, 0)

    @pl.when(is_hub)
    def _():
        pl.semaphore_signal(barrier, inc=1, device_id={"ep": other_hub})

    loads = [
        pltpu.make_async_copy(gate_hbm.at[0], w_gate, load_sems.at[0]),
        pltpu.make_async_copy(up_hbm.at[0], w_up, load_sems.at[1]),
        pltpu.make_async_copy(down_hbm.at[0], w_down, load_sems.at[2]),
    ]
    expert_at = lax.broadcasted_iota(jnp.int32, (devices, rows), 0)
    hits = [route_ids[k : k + 1, :] == expert_at for k in range(top)]
    named = sum(jnp.where(h, 1.0, 0.0) for h in hits)
    earlier = lax.broadcasted_iota(jnp.int32, (rows, rows), 0) < lax.broadcasted_iota(jnp.int32, (rows, rows), 1)
    ranked = dot32(named.astype(jnp.bfloat16), jnp.where(earlier, 1.0, 0.0).astype(jnp.bfloat16))
    base = ranked + (expert_at * capacity).astype(jnp.float32)
    gates = route_gates[...]
    weights = gates / jnp.sum(gates, axis=0, keepdims=True)
    for k in range(top):
        table[k : k + 1, :] = jnp.sum(jnp.where(hits[k], base, 0.0), axis=0, keepdims=True)
        table[top + k : top + k + 1, :] = weights[k : k + 1, :]
    token_load.wait()

    def norm(i, carry):
        at = pl.ds(pl.multiple_of(i * 64, 64), 64)
        floats = mixed[at, :].astype(jnp.float32)
        scale = lax.rsqrt(jnp.mean(floats * floats, axis=-1, keepdims=True) + EPS)
        value = (floats * scale * gain[...]).astype(jnp.bfloat16)
        for c in range(chunks):
            normed[c, at, :] = value[:, c * step : (c + 1) * step]
        return carry

    lax.fori_loop(0, rows // 64, norm, 0)

    @pl.when(is_hub)
    def _():
        pl.semaphore_wait(barrier, half)

    @pl.when(jnp.logical_not(is_hub))
    def _():
        pl.semaphore_wait(barrier, half - 1)

    def remote(src, dst, send, recv, device):
        return pltpu.make_async_remote_copy(
            src_ref=src, dst_ref=dst, send_sem=send, recv_sem=recv, device_id={"ep": device}
        )

    def table_copy(r, src, device):
        return remote(src, tables.at[r - 1], table_send.at[r - 1], table_recv.at[r - 1], device)

    def far_copy(r, c, src, device):
        return remote(src.at[c], far.at[r - 1, c], far_send.at[r - 1], far_recv.at[r - 1, c], device)

    def part_copy(k, c, src, slot, device):
        return remote(src.at[c], partial_in.at[slot, c], part_send.at[k], part_recv.at[slot, c], device)

    def span(i, part=0):
        return pl.ds(pl.multiple_of(part * unit + i * capacity, 16), capacity)

    def packs(r, c):
        return packed_near.at[c] if r == NEAR else packed.at[r, c]

    def returns(r, c):
        return backs_near.at[c] if r == NEAR else backs.at[r, c]

    def go_copy(r, c, part, i):
        target = (leaf if part else own) + i
        return remote(
            packs(r, c).at[span(i, part)], arrived.at[r, c, span(j)],
            go_send.at[r], go_recv.at[r], target,
        )

    def settle(r, every):
        count = unit if every else unit - capacity
        got = arrived.at[r, :, pl.ds(0, count)]
        remote(got, got, go_send.at[r], go_recv.at[r], peer).wait_recv()

    def go_sent(r):
        sent = packed_near.at[:, pl.ds(0, unit - capacity)] if r == NEAR else packed.at[r, :, pl.ds(0, 2 * unit - capacity)]
        remote(sent, sent, go_send.at[r], go_recv.at[r], peer).wait_send()

    def back_copy(r, c, i):
        return remote(
            arrived.at[r, c, span(i)], returns(r, c).at[span(j)],
            back_send.at[r], back_recv.at[r, c], own + i,
        )

    def back_sent(r):
        sent = arrived.at[r, :, pl.ds(0, unit - capacity)]
        remote(sent, sent, back_send.at[r], go_recv.at[r], peer).wait_send()

    def relay_copy(r, c):
        return remote(
            backs.at[r, c, pl.ds(0, unit)], backs.at[r, c, pl.ds(unit, unit)],
            relay_send.at[r], relay_recv.at[r, c], hub + j,
        )

    def others(act):
        def one(i, carry):
            act((j + 1 + i) % m)
            return carry

        lax.fori_loop(0, m - 1, one, 0)

    def everyone(act):
        def one(i, carry):
            act((j + i) % m)
            return carry

        lax.fori_loop(0, m, one, 0)

    def matrices(source, take, give, bases):
        width = 128

        def block(part, first):
            def one(i, carry):
                at = pl.multiple_of(part * unit + i * width, width)
                start = first * capacity + i * width
                slots = (start + lax.broadcasted_iota(jnp.int32, (width, rows), 0)).astype(jnp.float32)
                taken = jnp.zeros((width, rows), jnp.float32)
                total = jnp.zeros((width, rows), jnp.float32)
                for k in range(top):
                    hit = source[k : k + 1, :] == slots
                    taken = taken + jnp.where(hit, 1.0, 0.0)
                    total = total + jnp.where(hit, source[top + k : top + k + 1, :], 0.0)
                take[pl.ds(at, width), :] = taken.astype(jnp.bfloat16)
                give[:, pl.ds(at, width)] = total.T.astype(jnp.bfloat16)
                return carry

            lax.fori_loop(0, unit // width, one, 0)

        for part, first in enumerate(bases):
            block(part, first)

    def each(low, high, act):
        def one(c, carry):
            act(c)
            return carry

        lax.fori_loop(low, high, one, 0)

    def pack(r, c, source):
        take = take_near if r == NEAR else takes.at[r]
        target = packs(r, c)

        target[...] = dot32(take[...], source[c]).astype(jnp.bfloat16)
        if r != NEAR:
            everyone(lambda i: go_copy(r, c, 1, i).start())
        others(lambda i: go_copy(r, c, 0, i).start())
        arrived[r, c, span(j), :] = target[span(j), :]

    def hand_back(r, c):
        others(lambda i: back_copy(r, c, i).start())
        returns(r, c)[span(j), :] = arrived[r, c, span(j), :]

    def expert(r, send):
        def gated(i, carry):
            cols = pl.ds(pl.multiple_of(i * TILE, TILE), TILE)
            gate_pre = dot32(arrived[r, 0], w_gate[0:step, cols])
            up_pre = dot32(arrived[r, 0], w_up[0:step, cols])
            for c in range(1, chunks):
                gate_pre += dot32(arrived[r, c], w_gate[c * step : (c + 1) * step, cols])
                up_pre += dot32(arrived[r, c], w_up[c * step : (c + 1) * step, cols])
            hidden[:, cols] = (gate_pre / (1.0 + jnp.exp(-gate_pre)) * up_pre).astype(jnp.bfloat16)
            return carry

        lax.fori_loop(0, ff // TILE, gated, 0)

        def out(c):
            cols = pl.ds(pl.multiple_of(c * step, step), step)
            arrived[r, c] = dot32(hidden[...], w_down[:, cols]).astype(jnp.bfloat16)
            if send:
                hand_back(r, c)

        each(0, chunks, out)

    def out_copy(c):
        cols = pl.ds(pl.multiple_of(c * step, step), step)
        return pltpu.make_async_copy(mixed.at[:, cols], mixed_hbm.at[:, cols], out_sem)

    def finish(c, total):
        mixed[:, pl.ds(pl.multiple_of(c * step, step), step)] = total.astype(jnp.bfloat16)
        out_copy(c).start()

    def wait_back(r, c):
        got = returns(r, c).at[pl.ds(0, unit - capacity)]
        remote(got, got, back_send.at[r], back_recv.at[r, c], peer).wait_recv()

    def all_sent(sem, ref):
        remote(ref, ref, sem, go_recv.at[0], peer).wait_send()

    def hub_role():
        bases = (hub, leaf)
        lead = 2
        mid = chunks // 2

        def across_out(c):
            far_copy(ACROSS, c, normed, other_hub).start()

        each(0, lead, across_out)
        table_copy(ACROSS, table, other_hub).start()
        for load in loads:
            load.start()
        matrices(table, takes.at[HOME], gives.at[HOME], bases)
        table_copy(NEAR, table, leaf + j).wait_recv()
        table_copy(BEYOND, tables.at[NEAR - 1], other_hub).start()
        each(0, chunks, lambda c: pack(HOME, c, normed))
        matrices(tables.at[NEAR - 1], take_near, give_near, (own,))

        def near_in(c):
            far_copy(NEAR, c, normed, leaf + j).wait_recv()
            far_copy(BEYOND, c, far.at[NEAR - 1], other_hub).start()
            pack(NEAR, c, far.at[NEAR - 1])

        def far_in(r, c):
            far_copy(r, c, normed, other_hub).wait_recv()
            pack(r, c, far.at[r - 1])

        def merge(r, c):
            wait_back(r, c)
            relay_copy(r, c).wait_recv()
            far[r - 1, c] = dot32(gives[r], backs[r, c]).astype(jnp.bfloat16)
            slot = 0 if r == ACROSS else 1
            part_copy(slot, c, far.at[r - 1], slot, other_hub).start()

        def pass_on(c):
            wait_back(NEAR, c)
            part_copy(1, c, normed, 1, other_hub).wait_recv()
            total = dot32(give_near[...], backs_near[c]) + partial_in[1, c].astype(jnp.float32)
            far[NEAR - 1, c] = total.astype(jnp.bfloat16)
            part_copy(2, c, far.at[NEAR - 1], 1, leaf + j).start()

        def beyond_in(c):
            far_in(BEYOND, c)

        def across_in(c):
            far_in(ACROSS, c)

        each(0, lead, near_in)
        table_copy(ACROSS, table, other_hub).wait_recv()
        matrices(tables.at[ACROSS - 1], takes.at[ACROSS], gives.at[ACROSS], bases)
        table_copy(BEYOND, table, other_hub).wait_recv()
        matrices(tables.at[BEYOND - 1], takes.at[BEYOND], gives.at[BEYOND], bases)

        def early(c):
            beyond_in(c)
            near_in(c + lead)

        each(0, chunks - lead, early)
        each(lead, chunks, across_out)
        for load in loads:
            load.wait()
        settle(HOME, False)
        expert(HOME, False)
        each(chunks - lead, chunks, beyond_in)
        each(0, lead, across_in)
        settle(NEAR, False)
        expert(NEAR, False)
        settle(BEYOND, False)
        expert(BEYOND, True)
        each(lead, mid + 1, across_in)
        each(mid + 1, chunks - 1, across_in)
        merge(BEYOND, 0)
        across_in(chunks - 1)
        each(0, chunks, lambda c: hand_back(NEAR, c))
        each(1, mid, lambda c: merge(BEYOND, c))
        all_sent(far_send.at[BEYOND - 1], far.at[NEAR - 1])
        settle(ACROSS, False)
        expert(ACROSS, True)
        each(mid, chunks, lambda c: merge(BEYOND, c))
        each(0, chunks, lambda c: hand_back(HOME, c))
        each(0, mid, pass_on)

        def late(c):
            pass_on(c)
            merge(ACROSS, c - mid)

        each(mid, chunks, late)
        each(mid, chunks, lambda c: merge(ACROSS, c))
        all_sent(table_send.at[ACROSS - 1], table)
        all_sent(table_send.at[BEYOND - 1], table)
        all_sent(far_send.at[ACROSS - 1], normed)
        for r in range(4):
            go_sent(r)
            back_sent(r)

        def close(c):
            wait_back(HOME, c)
            relay_copy(HOME, c).wait_recv()
            part_copy(0, c, normed, 0, other_hub).wait_recv()
            finish(c, dot32(gives[HOME], backs[HOME, c]) + partial_in[0, c].astype(jnp.float32))

        each(0, chunks, close)
        for k in range(3):
            all_sent(part_send.at[k], normed)

    def leaf_role():
        lag = 2
        table_copy(NEAR, table, hub + j).start()
        each(0, chunks, lambda c: far_copy(NEAR, c, normed, hub + j).start())
        for load in loads:
            load.start()
        matrices(table, take_near, give_near, (own,))
        for load in loads:
            load.wait()

        def send_on(r, c):
            wait_back(r, c)
            relay_copy(r, c).start()

        settle(HOME, True)
        expert(HOME, True)
        each(0, chunks - lag, lambda c: send_on(HOME, c))
        settle(BEYOND, True)
        expert(BEYOND, True)
        each(0, chunks, lambda c: send_on(BEYOND, c))
        each(chunks - lag, chunks, lambda c: send_on(HOME, c))
        settle(ACROSS, True)
        expert(ACROSS, True)
        each(0, chunks, lambda c: pack(NEAR, c, normed))
        each(0, chunks, lambda c: send_on(ACROSS, c))
        settle(NEAR, False)
        expert(NEAR, True)
        all_sent(table_send.at[NEAR - 1], table)
        all_sent(far_send.at[NEAR - 1], normed)

        def close(c):
            wait_back(NEAR, c)
            part_copy(2, c, normed, 1, hub + j).wait_recv()
            finish(c, dot32(give_near[...], backs_near[c]) + partial_in[1, c].astype(jnp.float32))

        each(0, chunks, close)
        go_sent(NEAR)
        for r in range(4):
            back_sent(r)
        for r in (HOME, ACROSS, BEYOND):
            all_sent(relay_send.at[r], backs.at[r, :, pl.ds(0, unit)])

    @pl.when(is_hub)
    def _():
        hub_role()

    @pl.when(jnp.logical_not(is_hub))
    def _():
        leaf_role()

    pltpu.make_async_copy(mixed, mixed_hbm, out_sem).wait()


def body(tokens, norm_gain, route_ids, route_gates, w_gate, w_up, w_down):
    rows, width = tokens.shape
    top = route_ids.shape[1]
    devices = lax.axis_size("ep")
    experts = devices
    ff = w_gate.shape[2]
    capacity = 3 * rows * top // (2 * experts)
    m = devices // 4
    unit = m * capacity
    step = width // CHUNKS
    vmem = pl.BlockSpec(memory_space=pltpu.VMEM)
    hbm = pl.BlockSpec(memory_space=pl.ANY)
    bf16 = jnp.bfloat16
    dma = pltpu.SemaphoreType.DMA
    return pl.pallas_call(
        functools.partial(kernel, devices, capacity, top),
        out_shape=jax.ShapeDtypeStruct((rows, width), bf16),
        in_specs=[hbm, vmem, vmem, vmem, hbm, hbm, hbm],
        out_specs=hbm,
        scratch_shapes=[
            pltpu.VMEM((rows, width), bf16),
            pltpu.VMEM((2 * top, rows), jnp.float32),
            pltpu.VMEM((CHUNKS, rows, step), bf16),
            pltpu.VMEM((3, CHUNKS, rows, step), bf16),
            pltpu.VMEM((3, 2 * top, rows), jnp.float32),
            pltpu.VMEM((3, 2 * unit, rows), bf16),
            pltpu.VMEM((3, rows, 2 * unit), bf16),
            pltpu.VMEM((unit, rows), bf16),
            pltpu.VMEM((rows, unit), bf16),
            pltpu.VMEM((3, CHUNKS, 2 * unit, step), bf16),
            pltpu.VMEM((CHUNKS, unit, step), bf16),
            pltpu.VMEM((4, CHUNKS, unit, step), bf16),
            pltpu.VMEM((unit, ff), bf16),
            pltpu.VMEM((width, ff), bf16),
            pltpu.VMEM((width, ff), bf16),
            pltpu.VMEM((ff, width), bf16),
            pltpu.VMEM((3, CHUNKS, 2 * unit, step), bf16),
            pltpu.VMEM((CHUNKS, unit, step), bf16),
            pltpu.VMEM((2, CHUNKS, rows, step), bf16),
            dma((4,)),
            dma((3,)),
            dma((3,)),
            dma((3,)),
            dma((3, CHUNKS)),
            dma((4,)),
            dma((4,)),
            dma((4,)),
            dma((4, CHUNKS)),
            dma((3,)),
            dma((3, CHUNKS)),
            dma((3,)),
            dma((2, CHUNKS)),
            dma,
        ],
        compiler_params=pltpu.CompilerParams(
            collective_id=0, has_side_effects=True, vmem_limit_bytes=VMEM_BYTES
        ),
    )(tokens, norm_gain[None, :], route_ids.T, route_gates.T, w_gate, w_up, w_down)


def solution(mesh):
    placed = (
        P(("grp", "ep"), None),
        P(),
        P(("grp", "ep"), None),
        P(("grp", "ep"), None),
        P("ep", None, None),
        P("ep", None, None),
        P("ep", None, None),
    )
    return jax.shard_map(
        body, mesh=mesh, in_specs=placed, out_specs=P(("grp", "ep"), None), check_vma=False
    )
```

```python
import functools

import jax
import jax.numpy as jnp
from jax import lax
from jax.experimental import pallas as pl
from jax.experimental.pallas import tpu as pltpu
from jax.sharding import PartitionSpec as P

EPS = 1e-06
CHUNKS = 8
TILE = 256
VMEM_BYTES = 62000000


def dot32(a, b):
    return jnp.dot(a, b, preferred_element_type=jnp.float32)


HOME, ACROSS, BEYOND, NEAR = range(4)


def kernel(
    devices, capacity, top,
    tokens_hbm, gain_hbm, ids_hbm, gates_hbm, gate_hbm, up_hbm, down_hbm,
    mixed,
    gain, route_ids, route_gates, table, far, tables, takes, gives, take_near, give_near, packed, packed_near, arrived, hidden,
    w_gate, w_up, w_down, backs, backs_near, partial_in,
    load_sems, table_send, table_recv, far_send, far_recv, go_send, go_recv, back_send, back_recv,
    relay_send, relay_recv, part_send, part_recv,
):
    m = devices // 4
    half = 2 * m
    unit = m * capacity
    _, chunks, rows, step = far.shape
    ff = w_gate.shape[1]
    me = lax.axis_index("ep")
    side = me // half
    plane = me // m
    j = me % m
    q = me % half
    own = plane * m
    hub = (1 + side) * m
    leaf = 3 * side * m
    other_hub = (2 - side) * m + j
    peer = own + (j + 1) % m
    is_hub = plane * (3 - plane) > 0

    barrier = pltpu.get_barrier_semaphore()

    def greet(i, carry):
        pl.semaphore_signal(barrier, inc=1, device_id={"ep": side * half + (q + 1 + i) % half})
        return carry

    token_load = pltpu.make_async_copy(tokens_hbm, mixed, load_sems.at[3])
    small_loads = [
        pltpu.make_async_copy(ids_hbm, route_ids, load_sems.at[4]),
        pltpu.make_async_copy(gates_hbm, route_gates, load_sems.at[5]),
        pltpu.make_async_copy(gain_hbm, gain, load_sems.at[6]),
    ]
    token_load.start()
    for load in small_loads:
        load.start()
    lax.fori_loop(0, half - 1, greet, 0)

    @pl.when(is_hub)
    def _():
        pl.semaphore_signal(barrier, inc=1, device_id={"ep": other_hub})

    loads = [
        pltpu.make_async_copy(gate_hbm.at[0], w_gate, load_sems.at[0]),
        pltpu.make_async_copy(up_hbm.at[0], w_up, load_sems.at[1]),
        pltpu.make_async_copy(down_hbm.at[0], w_down, load_sems.at[2]),
    ]
    token_load.wait()

    @pl.when(is_hub)
    def _():
        pl.semaphore_wait(barrier, half)

    @pl.when(jnp.logical_not(is_hub))
    def _():
        pl.semaphore_wait(barrier, half - 1)

    def remote(src, dst, send, recv, device):
        return pltpu.make_async_remote_copy(
            src_ref=src, dst_ref=dst, send_sem=send, recv_sem=recv, device_id={"ep": device}
        )

    def raw(c):
        return mixed.at[:, pl.ds(pl.multiple_of(c * step, step), step)]

    def table_copy(r, src, device):
        return remote(src, tables.at[r - 1], table_send.at[r - 1], table_recv.at[r - 1], device)

    def far_copy(r, c, src, device):
        return remote(src, far.at[r - 1, c], far_send.at[r - 1], far_recv.at[r - 1, c], device)

    def part_copy(k, c, src, slot, device):
        return remote(src.at[c], partial_in.at[slot, c], part_send.at[k], part_recv.at[slot, c], device)

    def span(i, part=0):
        return pl.ds(pl.multiple_of(part * unit + i * capacity, 16), capacity)

    def packs(r, c):
        return packed_near.at[c] if r == NEAR else packed.at[r, c]

    def returns(r, c):
        return backs_near.at[c] if r == NEAR else backs.at[r, c]

    def go_copy(r, c, part, i):
        target = (leaf if part else own) + i
        return remote(
            packs(r, c).at[span(i, part)], arrived.at[r, c, span(j)],
            go_send.at[r], go_recv.at[r], target,
        )

    def settle(r, every):
        count = unit if every else unit - capacity
        got = arrived.at[r, :, pl.ds(0, count)]
        remote(got, got, go_send.at[r], go_recv.at[r], peer).wait_recv()

    def go_sent(r):
        sent = packed_near.at[:, pl.ds(0, unit - capacity)] if r == NEAR else packed.at[r, :, pl.ds(0, 2 * unit - capacity)]
        remote(sent, sent, go_send.at[r], go_recv.at[r], peer).wait_send()

    def back_copy(r, c, i):
        return remote(
            arrived.at[r, c, span(i)], returns(r, c).at[span(j)],
            back_send.at[r], back_recv.at[r, c], own + i,
        )

    def back_sent(r):
        sent = arrived.at[r, :, pl.ds(0, unit - capacity)]
        remote(sent, sent, back_send.at[r], go_recv.at[r], peer).wait_send()

    def relay_copy(r, c):
        return remote(
            backs.at[r, c, pl.ds(0, unit)], backs.at[r, c, pl.ds(unit, unit)],
            relay_send.at[r], relay_recv.at[r, c], hub + j,
        )

    def others(act):
        def one(i, carry):
            act((j + 1 + i) % m)
            return carry

        lax.fori_loop(0, m - 1, one, 0)

    def everyone(act):
        def one(i, carry):
            act((j + i) % m)
            return carry

        lax.fori_loop(0, m, one, 0)

    def matrices(source, take, give, bases):
        width = 128

        def block(part, first):
            def one(i, carry):
                at = pl.multiple_of(part * unit + i * width, width)
                start = first * capacity + i * width
                slots = (start + lax.broadcasted_iota(jnp.int32, (width, rows), 0)).astype(jnp.float32)
                taken = jnp.zeros((width, rows), jnp.float32)
                total = jnp.zeros((width, rows), jnp.float32)
                for k in range(top):
                    hit = source[k : k + 1, :] == slots
                    taken = taken + jnp.where(hit, 1.0, 0.0)
                    total = total + jnp.where(hit, source[top + k : top + k + 1, :], 0.0)
                take[pl.ds(at, width), :] = taken.astype(jnp.bfloat16)
                give[:, pl.ds(at, width)] = total.T.astype(jnp.bfloat16)
                return carry

            lax.fori_loop(0, unit // width, one, 0)

        for part, first in enumerate(bases):
            block(part, first)

    def build_table():
        for load in small_loads:
            load.wait()
        expert_at = lax.broadcasted_iota(jnp.int32, (devices, rows), 0)
        hits = [route_ids[k : k + 1, :] == expert_at for k in range(top)]
        named = sum(jnp.where(h, 1.0, 0.0) for h in hits)
        earlier = lax.broadcasted_iota(jnp.int32, (rows, rows), 0) < lax.broadcasted_iota(jnp.int32, (rows, rows), 1)
        ranked = dot32(named.astype(jnp.bfloat16), jnp.where(earlier, 1.0, 0.0).astype(jnp.bfloat16))
        base = ranked + (expert_at * capacity).astype(jnp.float32)
        gates = route_gates[...]
        weights = gates / jnp.sum(gates, axis=0, keepdims=True)
        for k in range(top):
            table[k : k + 1, :] = jnp.sum(jnp.where(hits[k], base, 0.0), axis=0, keepdims=True)
            table[top + k : top + k + 1, :] = weights[k : k + 1, :]

    def each(low, high, act):
        def one(c, carry):
            act(c)
            return carry

        lax.fori_loop(low, high, one, 0)

    def pack(r, c, source):
        take = take_near if r == NEAR else takes.at[r]
        target = packs(r, c)

        target[...] = dot32(take[...], source[...]).astype(jnp.bfloat16)
        if r != NEAR:
            everyone(lambda i: go_copy(r, c, 1, i).start())
        others(lambda i: go_copy(r, c, 0, i).start())
        arrived[r, c, span(j), :] = target[span(j), :]

    def hand_back(r, c):
        others(lambda i: back_copy(r, c, i).start())
        returns(r, c)[span(j), :] = arrived[r, c, span(j), :]

    def norm(r):
        block = 64

        def some(i, carry):
            at = pl.ds(pl.multiple_of(i * block, block), block)
            total = jnp.zeros((block, 1), jnp.float32)
            for c in range(chunks):
                floats = arrived[r, c, at, :].astype(jnp.float32)
                total += jnp.sum(floats * floats, axis=-1, keepdims=True)
            scale = lax.rsqrt(total / (chunks * step) + EPS)
            for c in range(chunks):
                floats = arrived[r, c, at, :].astype(jnp.float32)
                value = floats * scale * gain[:, c * step : (c + 1) * step]
                arrived[r, c, at, :] = value.astype(jnp.bfloat16)
            return carry

        lax.fori_loop(0, unit // block, some, 0)

    def expert(r, send):
        norm(r)

        def gated(i, carry):
            cols = pl.ds(pl.multiple_of(i * TILE, TILE), TILE)
            gate_pre = dot32(arrived[r, 0], w_gate[0:step, cols])
            up_pre = dot32(arrived[r, 0], w_up[0:step, cols])
            for c in range(1, chunks):
                gate_pre += dot32(arrived[r, c], w_gate[c * step : (c + 1) * step, cols])
                up_pre += dot32(arrived[r, c], w_up[c * step : (c + 1) * step, cols])
            hidden[:, cols] = (gate_pre / (1.0 + jnp.exp(-gate_pre)) * up_pre).astype(jnp.bfloat16)
            return carry

        lax.fori_loop(0, ff // TILE, gated, 0)

        def out(c):
            cols = pl.ds(pl.multiple_of(c * step, step), step)
            arrived[r, c] = dot32(hidden[...], w_down[:, cols]).astype(jnp.bfloat16)
            if send:
                hand_back(r, c)

        each(0, chunks, out)

    def finish(c, total):
        mixed[:, pl.ds(pl.multiple_of(c * step, step), step)] = total.astype(jnp.bfloat16)

    def wait_back(r, c):
        got = returns(r, c).at[pl.ds(0, unit - capacity)]
        remote(got, got, back_send.at[r], back_recv.at[r, c], peer).wait_recv()

    def all_sent(sem, ref):
        remote(ref, ref, sem, go_recv.at[0], peer).wait_send()

    def hub_role():
        bases = (hub, leaf)
        lead = 2
        mid = chunks // 2

        def across_out(c):
            far_copy(ACROSS, c, raw(c), other_hub).start()

        across_out(0)
        build_table()
        table_copy(ACROSS, table, other_hub).start()
        each(1, lead, across_out)
        for load in loads:
            load.start()
        matrices(table, takes.at[HOME], gives.at[HOME], bases)
        each(0, chunks, lambda c: pack(HOME, c, raw(c)))
        table_copy(NEAR, table, leaf + j).wait_recv()
        table_copy(BEYOND, tables.at[NEAR - 1], other_hub).start()
        matrices(tables.at[NEAR - 1], take_near, give_near, (own,))

        def near_in(c):
            far_copy(NEAR, c, raw(c), leaf + j).wait_recv()
            far_copy(BEYOND, c, far.at[NEAR - 1, c], other_hub).start()
            pack(NEAR, c, far.at[NEAR - 1, c])

        def far_in(r, c):
            far_copy(r, c, raw(c), other_hub).wait_recv()
            pack(r, c, far.at[r - 1, c])

        def merge(r, c):
            wait_back(r, c)
            relay_copy(r, c).wait_recv()
            far[r - 1, c] = dot32(gives[r], backs[r, c]).astype(jnp.bfloat16)
            slot = 0 if r == ACROSS else 1
            part_copy(slot, c, far.at[r - 1], slot, other_hub).start()

        def pass_on(c):
            wait_back(NEAR, c)
            part_copy(1, c, far.at[0], 1, other_hub).wait_recv()
            total = dot32(give_near[...], backs_near[c]) + partial_in[1, c].astype(jnp.float32)
            far[NEAR - 1, c] = total.astype(jnp.bfloat16)
            part_copy(2, c, far.at[NEAR - 1], 1, leaf + j).start()

        def beyond_in(c):
            far_in(BEYOND, c)

        def across_in(c):
            far_in(ACROSS, c)

        each(0, lead, near_in)
        table_copy(ACROSS, table, other_hub).wait_recv()
        matrices(tables.at[ACROSS - 1], takes.at[ACROSS], gives.at[ACROSS], bases)
        table_copy(BEYOND, table, other_hub).wait_recv()
        matrices(tables.at[BEYOND - 1], takes.at[BEYOND], gives.at[BEYOND], bases)

        def early(c):
            beyond_in(c)
            near_in(c + lead)

        each(0, chunks - lead, early)
        each(lead, chunks, across_out)
        for load in loads:
            load.wait()
        settle(HOME, False)
        expert(HOME, False)
        each(chunks - lead, chunks, beyond_in)
        each(0, lead, across_in)
        settle(NEAR, False)
        expert(NEAR, False)
        settle(BEYOND, False)
        expert(BEYOND, True)
        each(lead, mid + 1, across_in)
        each(mid + 1, chunks - 1, across_in)
        merge(BEYOND, 0)
        across_in(chunks - 1)
        each(0, chunks, lambda c: hand_back(NEAR, c))
        each(1, mid + lead, lambda c: merge(BEYOND, c))
        all_sent(far_send.at[BEYOND - 1], far.at[NEAR - 1])
        settle(ACROSS, False)
        expert(ACROSS, True)
        each(mid + lead, chunks, lambda c: merge(BEYOND, c))
        each(0, chunks, lambda c: hand_back(HOME, c))
        each(0, mid, pass_on)

        def late(c):
            pass_on(c)
            merge(ACROSS, c - mid)

        each(mid, chunks, late)
        each(mid, chunks, lambda c: merge(ACROSS, c))
        all_sent(table_send.at[ACROSS - 1], table)
        all_sent(table_send.at[BEYOND - 1], table)
        all_sent(far_send.at[ACROSS - 1], mixed)
        for r in range(4):
            go_sent(r)
            back_sent(r)

        def close(c):
            wait_back(HOME, c)
            relay_copy(HOME, c).wait_recv()
            part_copy(0, c, far.at[0], 0, other_hub).wait_recv()
            finish(c, dot32(gives[HOME], backs[HOME, c]) + partial_in[0, c].astype(jnp.float32))

        each(0, chunks, close)
        for k in range(3):
            all_sent(part_send.at[k], far.at[0])

    def leaf_role():
        lag = 2
        far_copy(NEAR, 0, raw(0), hub + j).start()
        build_table()
        table_copy(NEAR, table, hub + j).start()
        each(1, chunks, lambda c: far_copy(NEAR, c, raw(c), hub + j).start())
        for load in loads:
            load.start()
        matrices(table, take_near, give_near, (own,))
        for load in loads:
            load.wait()

        def send_on(r, c):
            wait_back(r, c)
            relay_copy(r, c).start()

        settle(HOME, True)
        expert(HOME, True)
        each(0, chunks - lag, lambda c: send_on(HOME, c))
        settle(BEYOND, True)
        expert(BEYOND, True)
        each(0, chunks, lambda c: send_on(BEYOND, c))
        each(chunks - lag, chunks, lambda c: send_on(HOME, c))
        settle(ACROSS, True)
        expert(ACROSS, True)
        each(0, chunks, lambda c: pack(NEAR, c, raw(c)))
        each(0, chunks, lambda c: send_on(ACROSS, c))
        settle(NEAR, False)
        expert(NEAR, True)
        all_sent(table_send.at[NEAR - 1], table)
        all_sent(far_send.at[NEAR - 1], mixed)

        def close(c):
            wait_back(NEAR, c)
            part_copy(2, c, far.at[0], 1, hub + j).wait_recv()
            finish(c, dot32(give_near[...], backs_near[c]) + partial_in[1, c].astype(jnp.float32))

        each(0, chunks, close)
        go_sent(NEAR)
        for r in range(4):
            back_sent(r)
        for r in (HOME, ACROSS, BEYOND):
            all_sent(relay_send.at[r], backs.at[r, :, pl.ds(0, unit)])

    @pl.when(is_hub)
    def _():
        hub_role()

    @pl.when(jnp.logical_not(is_hub))
    def _():
        leaf_role()


def body(tokens, norm_gain, route_ids, route_gates, w_gate, w_up, w_down):
    rows, width = tokens.shape
    top = route_ids.shape[1]
    devices = lax.axis_size("ep")
    experts = devices
    ff = w_gate.shape[2]
    capacity = 3 * rows * top // (2 * experts)
    m = devices // 4
    unit = m * capacity
    step = width // CHUNKS
    hbm = pl.BlockSpec(memory_space=pl.ANY)
    bf16 = jnp.bfloat16
    dma = pltpu.SemaphoreType.DMA
    return pl.pallas_call(
        functools.partial(kernel, devices, capacity, top),
        out_shape=pltpu.VMEM((rows, width), bf16),
        in_specs=[hbm] * 7,
        out_specs=pl.BlockSpec(memory_space=pltpu.VMEM),
        scratch_shapes=[
            pltpu.VMEM((1, width), jnp.float32),
            pltpu.VMEM((top, rows), jnp.int32),
            pltpu.VMEM((top, rows), jnp.float32),
            pltpu.VMEM((2 * top, rows), jnp.float32),
            pltpu.VMEM((3, CHUNKS, rows, step), bf16),
            pltpu.VMEM((3, 2 * top, rows), jnp.float32),
            pltpu.VMEM((3, 2 * unit, rows), bf16),
            pltpu.VMEM((3, rows, 2 * unit), bf16),
            pltpu.VMEM((unit, rows), bf16),
            pltpu.VMEM((rows, unit), bf16),
            pltpu.VMEM((3, CHUNKS, 2 * unit, step), bf16),
            pltpu.VMEM((CHUNKS, unit, step), bf16),
            pltpu.VMEM((4, CHUNKS, unit, step), bf16),
            pltpu.VMEM((unit, ff), bf16),
            pltpu.VMEM((width, ff), bf16),
            pltpu.VMEM((width, ff), bf16),
            pltpu.VMEM((ff, width), bf16),
            pltpu.VMEM((3, CHUNKS, 2 * unit, step), bf16),
            pltpu.VMEM((CHUNKS, unit, step), bf16),
            pltpu.VMEM((2, CHUNKS, rows, step), bf16),
            dma((7,)),
            dma((3,)),
            dma((3,)),
            dma((3,)),
            dma((3, CHUNKS)),
            dma((4,)),
            dma((4,)),
            dma((4,)),
            dma((4, CHUNKS)),
            dma((3,)),
            dma((3, CHUNKS)),
            dma((3,)),
            dma((2, CHUNKS)),
        ],
        compiler_params=pltpu.CompilerParams(
            collective_id=0, has_side_effects=True, vmem_limit_bytes=VMEM_BYTES
        ),
    )(tokens, norm_gain[None, :], route_ids.T, route_gates.T, w_gate, w_up, w_down)


def solution(mesh):
    placed = (
        P(("grp", "ep"), None),
        P(),
        P(("grp", "ep"), None),
        P(("grp", "ep"), None),
        P("ep", None, None),
        P("ep", None, None),
        P("ep", None, None),
    )
    return jax.shard_map(
        body, mesh=mesh, in_specs=placed, out_specs=P(("grp", "ep"), None), check_vma=False
    )
```

```python
import functools

import jax
import jax.numpy as jnp
from jax import lax
from jax.experimental import pallas as pl
from jax.experimental.pallas import tpu as pltpu
from jax.sharding import PartitionSpec as P

EPS = 1e-06
CHUNKS = 8
TILE = 256
VMEM_BYTES = 62000000


def dot32(a, b):
    return jnp.dot(a, b, preferred_element_type=jnp.float32)


HOME, ACROSS, BEYOND, NEAR = range(4)


def kernel(
    devices, capacity, top,
    tokens_hbm, gain_hbm, ids_hbm, gates_hbm, gate_hbm, up_hbm, down_hbm,
    mixed,
    gain, route_ids, route_gates, table, far, tables, takes, gives, take_near, give_near, packed, packed_near, arrived, hidden,
    w_gate, w_up, w_down, backs, backs_near, partial_in, local,
    load_sems, table_send, table_recv, far_send, far_recv, go_send, go_recv, back_send, back_recv,
    relay_send, relay_recv, part_send, part_recv, ready,
):
    m = devices // 4
    half = 2 * m
    unit = m * capacity
    _, chunks, rows, step = far.shape
    ff = w_gate.shape[1]
    me = lax.axis_index("ep")
    side = me // half
    plane = me // m
    j = me % m
    q = me % half
    own = plane * m
    hub = (1 + side) * m
    leaf = 3 * side * m
    other_hub = (2 - side) * m + j
    peer = own + (j + 1) % m
    is_hub = plane * (3 - plane) > 0

    barrier = pltpu.get_barrier_semaphore()

    @pl.when(is_hub)
    def _():
        pl.semaphore_signal(barrier, inc=1, device_id={"ep": other_hub})

    def greet(i, carry):
        pl.semaphore_signal(barrier, inc=1, device_id={"ep": leaf + (j + 1 + i) % m})
        return carry

    first_load = pltpu.make_async_copy(tokens_hbm.at[:, pl.ds(0, step)], mixed.at[:, pl.ds(0, step)], load_sems.at[7])
    token_load = pltpu.make_async_copy(
        tokens_hbm.at[:, pl.ds(step, (chunks - 1) * step)],
        mixed.at[:, pl.ds(step, (chunks - 1) * step)],
        load_sems.at[3],
    )
    small_loads = [
        pltpu.make_async_copy(ids_hbm, route_ids, load_sems.at[4]),
        pltpu.make_async_copy(gates_hbm, route_gates, load_sems.at[5]),
        pltpu.make_async_copy(gain_hbm, gain, load_sems.at[6]),
    ]
    first_load.start()
    token_load.start()
    for load in small_loads:
        load.start()
    lax.fori_loop(0, m - 1, greet, 0)

    @pl.when(is_hub)
    def _():
        pl.semaphore_signal(barrier, inc=1, device_id={"ep": leaf + j})

    loads = [
        pltpu.make_async_copy(gate_hbm.at[0], w_gate, load_sems.at[0]),
        pltpu.make_async_copy(up_hbm.at[0], w_up, load_sems.at[1]),
        pltpu.make_async_copy(down_hbm.at[0], w_down, load_sems.at[2]),
    ]
    first_load.wait()

    @pl.when(is_hub)
    def _():
        pl.semaphore_wait(barrier, 1)

    @pl.when(jnp.logical_not(is_hub))
    def _():
        pl.semaphore_wait(barrier, half - 1)

    def remote(src, dst, send, recv, device):
        return pltpu.make_async_remote_copy(
            src_ref=src, dst_ref=dst, send_sem=send, recv_sem=recv, device_id={"ep": device}
        )

    def raw(c):
        return mixed.at[:, pl.ds(pl.multiple_of(c * step, step), step)]

    def table_copy(r, src, device):
        return remote(src, tables.at[r - 1], table_send.at[r - 1], table_recv.at[r - 1], device)

    def far_copy(r, c, src, device):
        return remote(src, far.at[r - 1, c], far_send.at[r - 1], far_recv.at[r - 1, c], device)

    def part_copy(k, c, src, slot, device):
        return remote(src.at[c], partial_in.at[slot, c], part_send.at[k], part_recv.at[slot, c], device)

    def span(i, part=0):
        return pl.ds(pl.multiple_of(part * unit + i * capacity, 16), capacity)

    def packs(r, c):
        return packed_near.at[c] if r == NEAR else packed.at[r, c]

    def returns(r, c):
        return backs_near.at[c] if r == NEAR else backs.at[r, c]

    def go_copy(r, c, part, i):
        target = (leaf if part else own) + i
        return remote(
            packs(r, c).at[span(i, part)], arrived.at[r, c, span(j)],
            go_send.at[r], go_recv.at[r], target,
        )

    def settle(r, every):
        count = unit if every else unit - capacity
        got = arrived.at[r, :, pl.ds(0, count)]
        remote(got, got, go_send.at[r], go_recv.at[r], peer).wait_recv()

    def go_sent(r):
        sent = packed_near.at[:, pl.ds(0, unit - capacity)] if r == NEAR else packed.at[r, :, pl.ds(0, 2 * unit - capacity)]
        remote(sent, sent, go_send.at[r], go_recv.at[r], peer).wait_send()

    def back_copy(r, c, i):
        return remote(
            arrived.at[r, c, span(i)], returns(r, c).at[span(j)],
            back_send.at[r], back_recv.at[r, c], own + i,
        )

    def back_sent(r):
        sent = arrived.at[r, :, pl.ds(0, unit - capacity)]
        remote(sent, sent, back_send.at[r], go_recv.at[r], peer).wait_send()

    def relay_copy(r, c):
        return remote(
            backs.at[r, c, pl.ds(0, unit)], backs.at[r, c, pl.ds(unit, unit)],
            relay_send.at[r], relay_recv.at[r, c], hub + j,
        )

    def others(act):
        def one(i, carry):
            act((j + 1 + i) % m)
            return carry

        lax.fori_loop(0, m - 1, one, 0)

    def everyone(act):
        def one(i, carry):
            act((j + i) % m)
            return carry

        lax.fori_loop(0, m, one, 0)

    def matrices(source, take, give, bases):
        width = 128

        def block(part, first):
            def one(i, carry):
                at = pl.multiple_of(part * unit + i * width, width)
                start = first * capacity + i * width
                slots = (start + lax.broadcasted_iota(jnp.int32, (width, rows), 0)).astype(jnp.float32)
                taken = jnp.zeros((width, rows), jnp.float32)
                total = jnp.zeros((width, rows), jnp.float32)
                for k in range(top):
                    hit = source[k : k + 1, :] == slots
                    taken = taken + jnp.where(hit, 1.0, 0.0)
                    total = total + jnp.where(hit, source[top + k : top + k + 1, :], 0.0)
                take[pl.ds(at, width), :] = taken.astype(jnp.bfloat16)
                give[:, pl.ds(at, width)] = total.T.astype(jnp.bfloat16)
                return carry

            lax.fori_loop(0, unit // width, one, 0)

        for part, first in enumerate(bases):
            block(part, first)

    def build_table():
        for load in small_loads:
            load.wait()
        expert_at = lax.broadcasted_iota(jnp.int32, (devices, rows), 0)
        hits = [route_ids[k : k + 1, :] == expert_at for k in range(top)]
        named = sum(jnp.where(h, 1.0, 0.0) for h in hits)
        earlier = lax.broadcasted_iota(jnp.int32, (rows, rows), 0) < lax.broadcasted_iota(jnp.int32, (rows, rows), 1)
        ranked = dot32(named.astype(jnp.bfloat16), jnp.where(earlier, 1.0, 0.0).astype(jnp.bfloat16))
        base = ranked + (expert_at * capacity).astype(jnp.float32)
        gates = route_gates[...]
        weights = gates / jnp.sum(gates, axis=0, keepdims=True)
        for k in range(top):
            table[k : k + 1, :] = jnp.sum(jnp.where(hits[k], base, 0.0), axis=0, keepdims=True)
            table[top + k : top + k + 1, :] = weights[k : k + 1, :]

    def each(low, high, act):
        def one(c, carry):
            act(c)
            return carry

        lax.fori_loop(low, high, one, 0)

    def pack(r, c, source):
        take = take_near if r == NEAR else takes.at[r]
        target = packs(r, c)

        target[...] = dot32(take[...], source[...]).astype(jnp.bfloat16)
        if r != NEAR:
            everyone(lambda i: go_copy(r, c, 1, i).start())
        others(lambda i: go_copy(r, c, 0, i).start())
        arrived[r, c, span(j), :] = target[span(j), :]

    def hand_back(r, c):
        others(lambda i: back_copy(r, c, i).start())
        returns(r, c)[span(j), :] = arrived[r, c, span(j), :]

    def norm(r):
        block = 64

        def some(i, carry):
            at = pl.ds(pl.multiple_of(i * block, block), block)
            total = jnp.zeros((block, 1), jnp.float32)
            for c in range(chunks):
                floats = arrived[r, c, at, :].astype(jnp.float32)
                total += jnp.sum(floats * floats, axis=-1, keepdims=True)
            scale = lax.rsqrt(total / (chunks * step) + EPS)
            for c in range(chunks):
                floats = arrived[r, c, at, :].astype(jnp.float32)
                value = floats * scale * gain[:, c * step : (c + 1) * step]
                arrived[r, c, at, :] = value.astype(jnp.bfloat16)
            return carry

        lax.fori_loop(0, unit // block, some, 0)

    def expert(r, send):
        norm(r)

        def gated(i, carry):
            cols = pl.ds(pl.multiple_of(i * TILE, TILE), TILE)
            gate_pre = dot32(arrived[r, 0], w_gate[0:step, cols])
            up_pre = dot32(arrived[r, 0], w_up[0:step, cols])
            for c in range(1, chunks):
                gate_pre += dot32(arrived[r, c], w_gate[c * step : (c + 1) * step, cols])
                up_pre += dot32(arrived[r, c], w_up[c * step : (c + 1) * step, cols])
            hidden[:, cols] = (gate_pre / (1.0 + jnp.exp(-gate_pre)) * up_pre).astype(jnp.bfloat16)
            return carry

        lax.fori_loop(0, ff // TILE, gated, 0)

        def out(c):
            cols = pl.ds(pl.multiple_of(c * step, step), step)
            arrived[r, c] = dot32(hidden[...], w_down[:, cols]).astype(jnp.bfloat16)
            if send:
                hand_back(r, c)

        each(0, chunks, out)

    def finish(c, total):
        mixed[:, pl.ds(pl.multiple_of(c * step, step), step)] = total.astype(jnp.bfloat16)

    def wait_back(r, c):
        got = returns(r, c).at[pl.ds(0, unit - capacity)]
        remote(got, got, back_send.at[r], back_recv.at[r, c], peer).wait_recv()

    def all_sent(sem, ref):
        remote(ref, ref, sem, go_recv.at[0], peer).wait_send()

    def hub_role():
        bases = (hub, leaf)
        lead = 2
        mid = chunks // 2

        def across_out(c):
            far_copy(ACROSS, c, raw(c), other_hub).start()

        across_out(0)
        token_load.wait()
        build_table()
        table_copy(ACROSS, table, other_hub).start()
        each(1, lead, across_out)
        for load in loads:
            load.start()
        matrices(table, takes.at[HOME], gives.at[HOME], bases)
        pl.semaphore_wait(ready, m)
        each(0, chunks, lambda c: pack(HOME, c, raw(c)))
        table_copy(NEAR, table, leaf + j).wait_recv()
        table_copy(BEYOND, tables.at[NEAR - 1], other_hub).start()
        matrices(tables.at[NEAR - 1], take_near, give_near, (own,))

        def near_in(c):
            far_copy(NEAR, c, raw(c), leaf + j).wait_recv()
            far_copy(BEYOND, c, far.at[NEAR - 1, c], other_hub).start()
            pack(NEAR, c, far.at[NEAR - 1, c])

        def far_in(r, c):
            far_copy(r, c, raw(c), other_hub).wait_recv()
            pack(r, c, far.at[r - 1, c])

        def merge(r, c):
            wait_back(r, c)
            relay_copy(r, c).wait_recv()
            far[r - 1, c] = dot32(gives[r], backs[r, c]).astype(jnp.bfloat16)
            slot = 0 if r == ACROSS else 1
            part_copy(slot, c, far.at[r - 1], slot, other_hub).start()

        def pass_on(c):
            wait_back(NEAR, c)
            part_copy(1, c, far.at[0], 1, other_hub).wait_recv()
            total = dot32(give_near[...], backs_near[c]) + partial_in[1, c].astype(jnp.float32)
            far[NEAR - 1, c] = total.astype(jnp.bfloat16)
            part_copy(2, c, far.at[NEAR - 1], 1, leaf + j).start()

        def beyond_in(c):
            far_in(BEYOND, c)

        def across_in(c):
            far_in(ACROSS, c)

        each(0, lead, near_in)
        table_copy(ACROSS, table, other_hub).wait_recv()
        matrices(tables.at[ACROSS - 1], takes.at[ACROSS], gives.at[ACROSS], bases)
        table_copy(BEYOND, table, other_hub).wait_recv()
        matrices(tables.at[BEYOND - 1], takes.at[BEYOND], gives.at[BEYOND], bases)

        def early(c):
            beyond_in(c)
            near_in(c + lead)

        each(0, chunks - lead, early)
        each(lead, chunks, across_out)
        for load in loads:
            load.wait()
        settle(HOME, False)
        expert(HOME, False)
        each(chunks - lead, chunks, beyond_in)
        each(0, lead, across_in)
        settle(NEAR, False)
        expert(NEAR, False)
        settle(BEYOND, False)
        expert(BEYOND, True)
        each(lead, mid + 1, across_in)
        each(mid + 1, chunks - 1, across_in)
        merge(BEYOND, 0)
        across_in(chunks - 1)
        each(0, chunks, lambda c: hand_back(NEAR, c))
        each(1, mid + lead, lambda c: merge(BEYOND, c))
        all_sent(far_send.at[BEYOND - 1], far.at[NEAR - 1])
        settle(ACROSS, False)
        expert(ACROSS, True)
        each(mid + lead, chunks, lambda c: merge(BEYOND, c))
        each(0, chunks, lambda c: hand_back(HOME, c))
        each(0, mid, pass_on)

        def late(c):
            pass_on(c)
            merge(ACROSS, c - mid)

        each(mid, chunks, late)
        each(mid, chunks, lambda c: merge(ACROSS, c))
        all_sent(table_send.at[ACROSS - 1], table)
        all_sent(table_send.at[BEYOND - 1], table)
        all_sent(far_send.at[ACROSS - 1], mixed)
        for r in range(4):
            go_sent(r)
            back_sent(r)

        def close(c):
            wait_back(HOME, c)
            relay_copy(HOME, c).wait_recv()
            local[...] = dot32(gives[HOME], backs[HOME, c])
            part_copy(0, c, far.at[0], 0, other_hub).wait_recv()
            finish(c, local[...] + partial_in[0, c].astype(jnp.float32))

        each(0, chunks, close)
        for k in range(3):
            all_sent(part_send.at[k], far.at[0])

    def leaf_role():
        lag = 2
        far_copy(NEAR, 0, raw(0), hub + j).start()
        each(0, m, lambda i: pl.semaphore_signal(ready, inc=1, device_id={"ep": hub + (j + i) % m}))
        token_load.wait()
        build_table()
        table_copy(NEAR, table, hub + j).start()
        each(1, chunks, lambda c: far_copy(NEAR, c, raw(c), hub + j).start())
        for load in loads:
            load.start()
        matrices(table, take_near, give_near, (own,))
        for load in loads:
            load.wait()

        def send_on(r, c):
            wait_back(r, c)
            relay_copy(r, c).start()

        settle(HOME, True)
        expert(HOME, True)
        each(0, chunks - lag, lambda c: send_on(HOME, c))
        settle(BEYOND, True)
        expert(BEYOND, True)
        each(0, chunks, lambda c: send_on(BEYOND, c))
        each(chunks - lag, chunks, lambda c: send_on(HOME, c))
        settle(ACROSS, True)
        expert(ACROSS, True)
        each(0, chunks, lambda c: pack(NEAR, c, raw(c)))
        each(0, chunks, lambda c: send_on(ACROSS, c))
        settle(NEAR, False)
        expert(NEAR, True)
        all_sent(table_send.at[NEAR - 1], table)
        all_sent(far_send.at[NEAR - 1], mixed)

        def close(c):
            wait_back(NEAR, c)
            part_copy(2, c, far.at[0], 1, hub + j).wait_recv()
            finish(c, dot32(give_near[...], backs_near[c]) + partial_in[1, c].astype(jnp.float32))

        each(0, chunks, close)
        go_sent(NEAR)
        for r in range(4):
            back_sent(r)
        for r in (HOME, ACROSS, BEYOND):
            all_sent(relay_send.at[r], backs.at[r, :, pl.ds(0, unit)])

    @pl.when(is_hub)
    def _():
        hub_role()

    @pl.when(jnp.logical_not(is_hub))
    def _():
        leaf_role()


def body(tokens, norm_gain, route_ids, route_gates, w_gate, w_up, w_down):
    rows, width = tokens.shape
    top = route_ids.shape[1]
    devices = lax.axis_size("ep")
    experts = devices
    ff = w_gate.shape[2]
    capacity = 3 * rows * top // (2 * experts)
    m = devices // 4
    unit = m * capacity
    step = width // CHUNKS
    hbm = pl.BlockSpec(memory_space=pl.ANY)
    bf16 = jnp.bfloat16
    dma = pltpu.SemaphoreType.DMA
    return pl.pallas_call(
        functools.partial(kernel, devices, capacity, top),
        out_shape=pltpu.VMEM((rows, width), bf16),
        in_specs=[hbm] * 7,
        out_specs=pl.BlockSpec(memory_space=pltpu.VMEM),
        scratch_shapes=[
            pltpu.VMEM((1, width), jnp.float32),
            pltpu.VMEM((top, rows), jnp.int32),
            pltpu.VMEM((top, rows), jnp.float32),
            pltpu.VMEM((2 * top, rows), jnp.float32),
            pltpu.VMEM((3, CHUNKS, rows, step), bf16),
            pltpu.VMEM((3, 2 * top, rows), jnp.float32),
            pltpu.VMEM((3, 2 * unit, rows), bf16),
            pltpu.VMEM((3, rows, 2 * unit), bf16),
            pltpu.VMEM((unit, rows), bf16),
            pltpu.VMEM((rows, unit), bf16),
            pltpu.VMEM((3, CHUNKS, 2 * unit, step), bf16),
            pltpu.VMEM((CHUNKS, unit, step), bf16),
            pltpu.VMEM((4, CHUNKS, unit, step), bf16),
            pltpu.VMEM((unit, ff), bf16),
            pltpu.VMEM((width, ff), bf16),
            pltpu.VMEM((width, ff), bf16),
            pltpu.VMEM((ff, width), bf16),
            pltpu.VMEM((3, CHUNKS, 2 * unit, step), bf16),
            pltpu.VMEM((CHUNKS, unit, step), bf16),
            pltpu.VMEM((2, CHUNKS, rows, step), bf16),
            pltpu.VMEM((rows, step), jnp.float32),
            dma((8,)),
            dma((3,)),
            dma((3,)),
            dma((3,)),
            dma((3, CHUNKS)),
            dma((4,)),
            dma((4,)),
            dma((4,)),
            dma((4, CHUNKS)),
            dma((3,)),
            dma((3, CHUNKS)),
            dma((3,)),
            dma((2, CHUNKS)),
            pltpu.SemaphoreType.REGULAR,
        ],
        compiler_params=pltpu.CompilerParams(
            collective_id=0, has_side_effects=True, vmem_limit_bytes=VMEM_BYTES
        ),
    )(tokens, norm_gain[None, :], route_ids.T, route_gates.T, w_gate, w_up, w_down)


def solution(mesh):
    placed = (
        P(("grp", "ep"), None),
        P(),
        P(("grp", "ep"), None),
        P(("grp", "ep"), None),
        P("ep", None, None),
        P("ep", None, None),
        P("ep", None, None),
    )
    return jax.shard_map(
        body, mesh=mesh, in_specs=placed, out_specs=P(("grp", "ep"), None), check_vma=False
    )
```

```python
import functools

import jax
import jax.numpy as jnp
from jax import lax
from jax.experimental import pallas as pl
from jax.experimental.pallas import tpu as pltpu
from jax.sharding import PartitionSpec as P

EPS = 1e-06
CHUNKS = 8
TILE = 256
VMEM_BYTES = 62000000


def dot32(a, b):
    return jnp.dot(a, b, preferred_element_type=jnp.float32)


HOME, ACROSS, BEYOND, NEAR = range(4)


def kernel(
    devices, capacity, top,
    tokens_hbm, gain_hbm, ids_hbm, gates_hbm, gate_hbm, up_hbm, down_hbm,
    mixed,
    gain, route_ids, route_gates, table, far, tables, takes, gives, take_near, give_near, packed, packed_near, arrived, hidden,
    w_gate, w_up, w_down, backs, backs_near, partial_in, local,
    load_sems, table_send, table_recv, far_send, far_recv, go_send, go_recv, back_send, back_recv,
    relay_send, relay_recv, part_send, part_recv, ready,
):
    m = devices // 4
    half = 2 * m
    unit = m * capacity
    _, chunks, rows, step = far.shape
    ff = w_gate.shape[1]
    me = lax.axis_index("ep")
    side = me // half
    plane = me // m
    j = me % m
    q = me % half
    own = plane * m
    hub = (1 + side) * m
    leaf = 3 * side * m
    other_hub = (2 - side) * m + j
    peer = own + (j + 1) % m
    is_hub = plane * (3 - plane) > 0

    barrier = pltpu.get_barrier_semaphore()

    @pl.when(is_hub)
    def _():
        pl.semaphore_signal(barrier, inc=1, device_id={"ep": other_hub})

    def greet(i, carry):
        pl.semaphore_signal(barrier, inc=1, device_id={"ep": leaf + (j + 1 + i) % m})
        return carry

    first_load = pltpu.make_async_copy(tokens_hbm.at[:, pl.ds(0, step)], mixed.at[:, pl.ds(0, step)], load_sems.at[7])
    token_load = pltpu.make_async_copy(
        tokens_hbm.at[:, pl.ds(step, (chunks - 1) * step)],
        mixed.at[:, pl.ds(step, (chunks - 1) * step)],
        load_sems.at[3],
    )
    small_loads = [
        pltpu.make_async_copy(ids_hbm, route_ids, load_sems.at[4]),
        pltpu.make_async_copy(gates_hbm, route_gates, load_sems.at[5]),
        pltpu.make_async_copy(gain_hbm, gain, load_sems.at[6]),
    ]
    first_load.start()
    token_load.start()
    for load in small_loads:
        load.start()
    lax.fori_loop(0, m - 1, greet, 0)

    @pl.when(is_hub)
    def _():
        pl.semaphore_signal(barrier, inc=1, device_id={"ep": leaf + j})

    loads = [
        pltpu.make_async_copy(gate_hbm.at[0], w_gate, load_sems.at[0]),
        pltpu.make_async_copy(up_hbm.at[0], w_up, load_sems.at[1]),
        pltpu.make_async_copy(down_hbm.at[0], w_down, load_sems.at[2]),
    ]
    first_load.wait()

    @pl.when(is_hub)
    def _():
        pl.semaphore_wait(barrier, 1)

    @pl.when(jnp.logical_not(is_hub))
    def _():
        pl.semaphore_wait(barrier, half - 1)

    def remote(src, dst, send, recv, device):
        return pltpu.make_async_remote_copy(
            src_ref=src, dst_ref=dst, send_sem=send, recv_sem=recv, device_id={"ep": device}
        )

    def raw(c):
        return mixed.at[:, pl.ds(pl.multiple_of(c * step, step), step)]

    def table_copy(r, src, device):
        return remote(src, tables.at[r - 1], table_send, table_recv.at[r - 1], device)

    def far_slot(r, c):
        return far_recv.at[2 * chunks + c if r == ACROSS else (r - BEYOND) * chunks + c]

    def far_copy(r, c, src, device, group=None):
        send = far_send.at[1 if r == BEYOND else 0]
        return remote(src, far.at[r - 1, c], send, far_slot(r, c if group is None else group), device)

    def part_slot(slot, c):
        return part_recv.at[chunks // 2 + 1 + c // 2 if slot else c // 2 + c // (chunks - 1)]

    def part_copy(c, src, slot, device):
        return remote(src.at[c], partial_in.at[slot, c], part_send, part_slot(slot, c), device)

    def part_wait(slot, c, count):
        got = partial_in.at[slot, pl.ds(c, count)]
        remote(got, got, part_send, part_slot(slot, c), peer).wait_recv()

    def span(i, part=0):
        return pl.ds(pl.multiple_of(part * unit + i * capacity, 16), capacity)

    def packs(r, c):
        return packed_near.at[c] if r == NEAR else packed.at[r, c]

    def returns(r, c):
        return backs_near.at[c] if r == NEAR else backs.at[r, c]

    def go_copy(r, c, part, i):
        target = (leaf if part else own) + i
        return remote(
            packs(r, c).at[span(i, part)], arrived.at[r, c, span(j)],
            go_send.at[r // NEAR], go_recv.at[r], target,
        )

    def settle(r, every):
        count = unit if every else unit - capacity
        got = arrived.at[r, :, pl.ds(0, count)]
        remote(got, got, go_send.at[0], go_recv.at[r], peer).wait_recv()

    def go_sent(near):
        sent = packed_near.at[:, pl.ds(0, unit - capacity)] if near else packed.at[:, :, pl.ds(0, 2 * unit - capacity)]
        remote(sent, sent, go_send.at[near], go_recv.at[0], peer).wait_send()

    def back_slot(r, c):
        if r == HOME:
            return back_recv.at[c // 2]
        if r == NEAR:
            return back_recv.at[chunks // 2 + 2 * chunks]
        return back_recv.at[chunks // 2 + (r - ACROSS) * chunks + c]

    def back_copy(r, c, i):
        return remote(
            arrived.at[r, c, span(i)], returns(r, c).at[span(j)],
            back_send, back_slot(r, c), own + i,
        )

    def back_sent():
        sent = arrived.at[:, :, pl.ds(0, unit - capacity)]
        remote(sent, sent, back_send, go_recv.at[0], peer).wait_send()

    def relay_copy(r, c):
        return remote(
            backs.at[r, c, pl.ds(0, unit)], backs.at[r, c, pl.ds(unit, unit)],
            relay_send, relay_recv.at[0 if r == HOME else 1 + (r - ACROSS) * chunks + c], hub + j,
        )

    def others(act):
        def one(i, carry):
            act((j + 1 + i) % m)
            return carry

        lax.fori_loop(0, m - 1, one, 0)

    def everyone(act):
        def one(i, carry):
            act((j + i) % m)
            return carry

        lax.fori_loop(0, m, one, 0)

    def matrices(source, take, give, bases):
        width = 128

        def block(part, first):
            def one(i, carry):
                at = pl.multiple_of(part * unit + i * width, width)
                start = first * capacity + i * width
                slots = (start + lax.broadcasted_iota(jnp.int32, (width, rows), 0)).astype(jnp.float32)
                taken = jnp.zeros((width, rows), jnp.float32)
                total = jnp.zeros((width, rows), jnp.float32)
                for k in range(top):
                    hit = source[k : k + 1, :] == slots
                    taken = taken + jnp.where(hit, 1.0, 0.0)
                    total = total + jnp.where(hit, source[top + k : top + k + 1, :], 0.0)
                take[pl.ds(at, width), :] = taken.astype(jnp.bfloat16)
                give[:, pl.ds(at, width)] = total.T.astype(jnp.bfloat16)
                return carry

            lax.fori_loop(0, unit // width, one, 0)

        for part, first in enumerate(bases):
            block(part, first)

    def build_table():
        for load in small_loads:
            load.wait()
        expert_at = lax.broadcasted_iota(jnp.int32, (devices, rows), 0)
        hits = [route_ids[k : k + 1, :] == expert_at for k in range(top)]
        named = sum(jnp.where(h, 1.0, 0.0) for h in hits)
        earlier = lax.broadcasted_iota(jnp.int32, (rows, rows), 0) < lax.broadcasted_iota(jnp.int32, (rows, rows), 1)
        ranked = dot32(named.astype(jnp.bfloat16), jnp.where(earlier, 1.0, 0.0).astype(jnp.bfloat16))
        base = ranked + (expert_at * capacity).astype(jnp.float32)
        gates = route_gates[...]
        weights = gates / jnp.sum(gates, axis=0, keepdims=True)
        for k in range(top):
            table[k : k + 1, :] = jnp.sum(jnp.where(hits[k], base, 0.0), axis=0, keepdims=True)
            table[top + k : top + k + 1, :] = weights[k : k + 1, :]

    def each(low, high, act):
        def one(c, carry):
            act(c)
            return carry

        lax.fori_loop(low, high, one, 0)

    def pack(r, c, source):
        take = take_near if r == NEAR else takes.at[r]
        target = packs(r, c)

        target[...] = dot32(take[...], source[...]).astype(jnp.bfloat16)
        if r != NEAR:
            everyone(lambda i: go_copy(r, c, 1, i).start())
        others(lambda i: go_copy(r, c, 0, i).start())
        arrived[r, c, span(j), :] = target[span(j), :]

    def hand_back(r, c):
        others(lambda i: back_copy(r, c, i).start())
        returns(r, c)[span(j), :] = arrived[r, c, span(j), :]

    def norm(r):
        block = 64

        def some(i, carry):
            at = pl.ds(pl.multiple_of(i * block, block), block)
            total = jnp.zeros((block, 1), jnp.float32)
            for c in range(chunks):
                floats = arrived[r, c, at, :].astype(jnp.float32)
                total += jnp.sum(floats * floats, axis=-1, keepdims=True)
            scale = lax.rsqrt(total / (chunks * step) + EPS)
            for c in range(chunks):
                floats = arrived[r, c, at, :].astype(jnp.float32)
                value = floats * scale * gain[:, c * step : (c + 1) * step]
                arrived[r, c, at, :] = value.astype(jnp.bfloat16)
            return carry

        lax.fori_loop(0, unit // block, some, 0)

    def expert(r, send):
        norm(r)

        def gated(i, carry):
            cols = pl.ds(pl.multiple_of(i * TILE, TILE), TILE)
            gate_pre = dot32(arrived[r, 0], w_gate[0:step, cols])
            up_pre = dot32(arrived[r, 0], w_up[0:step, cols])
            for c in range(1, chunks):
                gate_pre += dot32(arrived[r, c], w_gate[c * step : (c + 1) * step, cols])
                up_pre += dot32(arrived[r, c], w_up[c * step : (c + 1) * step, cols])
            hidden[:, cols] = (gate_pre / (1.0 + jnp.exp(-gate_pre)) * up_pre).astype(jnp.bfloat16)
            return carry

        lax.fori_loop(0, ff // TILE, gated, 0)

        def out(c):
            cols = pl.ds(pl.multiple_of(c * step, step), step)
            arrived[r, c] = dot32(hidden[...], w_down[:, cols]).astype(jnp.bfloat16)
            if send:
                hand_back(r, c)

        each(0, chunks, out)

    def finish(c, total):
        mixed[:, pl.ds(pl.multiple_of(c * step, step), step)] = total.astype(jnp.bfloat16)

    def wait_back(r, c):
        got = returns(r, c).at[pl.ds(0, unit - capacity)]
        remote(got, got, back_send, back_slot(r, c), peer).wait_recv()

    def wait_home(p):
        got = backs.at[HOME, pl.ds(2 * p, 2), pl.ds(0, unit - capacity)]
        remote(got, got, back_send, back_slot(HOME, 2 * p), peer).wait_recv()

    def wait_near():
        got = backs_near.at[:, pl.ds(0, unit - capacity)]
        remote(got, got, back_send, back_slot(NEAR, 0), peer).wait_recv()

    def all_sent(sem, ref):
        remote(ref, ref, sem, go_recv.at[0], peer).wait_send()

    def hub_role():
        bases = (hub, leaf)
        lead = 2
        mid = chunks // 2

        def across_out(c, group):
            far_copy(ACROSS, c, raw(c), other_hub, group).start()

        across_out(0, 0)
        token_load.wait()
        build_table()
        table_copy(ACROSS, table, other_hub).start()
        each(1, lead, lambda c: across_out(c, 0))
        for load in loads:
            load.start()
        matrices(table, takes.at[HOME], gives.at[HOME], bases)
        pl.semaphore_wait(ready, m)
        each(0, chunks, lambda c: pack(HOME, c, raw(c)))
        table_copy(NEAR, table, leaf + j).wait_recv()
        table_copy(BEYOND, tables.at[NEAR - 1], other_hub).start()
        matrices(tables.at[NEAR - 1], take_near, give_near, (own,))

        def near_in(c):
            far_copy(NEAR, c, raw(c), leaf + j).wait_recv()
            far_copy(BEYOND, c, far.at[NEAR - 1, c], other_hub).start()
            pack(NEAR, c, far.at[NEAR - 1, c])

        def far_in(r, c):
            far_copy(r, c, raw(c), other_hub).wait_recv()
            pack(r, c, far.at[r - 1, c])

        def merge(r, c):
            wait_back(r, c)
            relay_copy(r, c).wait_recv()
            far[r - 1, c] = dot32(gives[r], backs[r, c]).astype(jnp.bfloat16)
            part_copy(c, far.at[r - 1], 0 if r == ACROSS else 1, other_hub).start()

        def pass_on(p):
            part_wait(1, 2 * p, 2)

            def one(c):
                total = dot32(give_near[...], backs_near[c]) + partial_in[1, c].astype(jnp.float32)
                far[NEAR - 1, c] = total.astype(jnp.bfloat16)
                part_copy(c, far.at[NEAR - 1], 1, leaf + j).start()

            each(2 * p, 2 * p + 2, one)

        def beyond_in(c):
            far_in(BEYOND, c)

        def across_in(low, count, group):
            got = far.at[ACROSS - 1, pl.ds(low, count)]
            remote(got, got, far_send.at[0], far_slot(ACROSS, group), peer).wait_recv()
            each(low, low + count, lambda c: pack(ACROSS, c, far.at[ACROSS - 1, c]))

        def across_one(c):
            across_in(c, 1, c - mid + 1)

        each(0, lead, near_in)
        table_copy(ACROSS, table, other_hub).wait_recv()
        matrices(tables.at[ACROSS - 1], takes.at[ACROSS], gives.at[ACROSS], bases)
        table_copy(BEYOND, table, other_hub).wait_recv()
        matrices(tables.at[BEYOND - 1], takes.at[BEYOND], gives.at[BEYOND], bases)

        def early(c):
            beyond_in(c)
            near_in(c + lead)

        each(0, chunks - lead, early)
        each(lead, mid + 1, lambda c: across_out(c, 1))
        each(mid + 1, chunks, lambda c: across_out(c, c - mid + 1))
        for load in loads:
            load.wait()
        settle(HOME, False)
        expert(HOME, False)
        each(chunks - lead, chunks, beyond_in)
        across_in(0, lead, 0)
        settle(NEAR, False)
        expert(NEAR, False)
        settle(BEYOND, False)
        expert(BEYOND, True)
        across_in(lead, mid + 1 - lead, 1)
        each(mid + 1, chunks - 1, across_one)
        merge(BEYOND, 0)
        across_one(chunks - 1)
        each(0, chunks, lambda c: hand_back(NEAR, c))
        each(1, mid + lead, lambda c: merge(BEYOND, c))
        all_sent(far_send.at[1], far.at[NEAR - 1])
        settle(ACROSS, False)
        expert(ACROSS, True)
        each(mid + lead, chunks, lambda c: merge(BEYOND, c))
        each(0, chunks, lambda c: hand_back(HOME, c))
        wait_near()
        each(0, mid // 2, pass_on)

        def late(p):
            pass_on(p)
            each(2 * p - mid, 2 * p - mid + 2, lambda c: merge(ACROSS, c))

        each(mid // 2, chunks // 2, late)
        each(mid, chunks, lambda c: merge(ACROSS, c))
        all_sent(table_send, tables.at[pl.ds(0, 2)])
        all_sent(far_send.at[0], mixed)
        go_sent(0)
        go_sent(1)
        back_sent()
        each(0, chunks // 2, wait_home)
        got = backs.at[HOME, :, pl.ds(0, unit)]
        remote(got, got, relay_send, relay_recv.at[0], peer).wait_recv()

        def close(c, wait):
            local[...] = dot32(gives[HOME], backs[HOME, c])
            wait()
            finish(c, local[...] + partial_in[0, c].astype(jnp.float32))

        def close_pair(p):
            close(2 * p, lambda: part_wait(0, 2 * p, 2))
            close(2 * p + 1, lambda: None)

        each(0, chunks // 2 - 1, close_pair)
        each(chunks - 2, chunks, lambda c: close(c, lambda: part_wait(0, c, 1)))
        all_sent(part_send, far)

    def leaf_role():
        far_copy(NEAR, 0, raw(0), hub + j).start()
        each(0, m, lambda i: pl.semaphore_signal(ready, inc=1, device_id={"ep": hub + (j + i) % m}))
        token_load.wait()
        build_table()
        table_copy(NEAR, table, hub + j).start()
        each(1, chunks, lambda c: far_copy(NEAR, c, raw(c), hub + j).start())
        for load in loads:
            load.start()
        matrices(table, take_near, give_near, (own,))
        for load in loads:
            load.wait()

        def send_on(r, c):
            wait_back(r, c)
            relay_copy(r, c).start()

        def send_home(p):
            wait_home(p)
            each(2 * p, 2 * p + 2, lambda c: relay_copy(HOME, c).start())

        settle(HOME, True)
        expert(HOME, True)
        each(0, chunks // 2 - 1, send_home)
        settle(BEYOND, True)
        expert(BEYOND, True)
        each(0, chunks, lambda c: send_on(BEYOND, c))
        send_home(chunks // 2 - 1)
        settle(ACROSS, True)
        expert(ACROSS, True)
        each(0, chunks, lambda c: pack(NEAR, c, raw(c)))
        each(0, chunks, lambda c: send_on(ACROSS, c))
        settle(NEAR, False)
        expert(NEAR, True)
        all_sent(table_send, table)
        all_sent(far_send.at[0], mixed)

        wait_near()

        def close_pair(p):
            part_wait(1, 2 * p, 2)
            for c in (2 * p, 2 * p + 1):
                finish(c, dot32(give_near[...], backs_near[c]) + partial_in[1, c].astype(jnp.float32))

        each(0, chunks // 2, close_pair)
        go_sent(1)
        back_sent()
        all_sent(relay_send, backs.at[:, :, pl.ds(0, unit)])

    @pl.when(is_hub)
    def _():
        hub_role()

    @pl.when(jnp.logical_not(is_hub))
    def _():
        leaf_role()


def body(tokens, norm_gain, route_ids, route_gates, w_gate, w_up, w_down):
    rows, width = tokens.shape
    top = route_ids.shape[1]
    devices = lax.axis_size("ep")
    experts = devices
    ff = w_gate.shape[2]
    capacity = 3 * rows * top // (2 * experts)
    m = devices // 4
    unit = m * capacity
    step = width // CHUNKS
    hbm = pl.BlockSpec(memory_space=pl.ANY)
    bf16 = jnp.bfloat16
    dma = pltpu.SemaphoreType.DMA
    return pl.pallas_call(
        functools.partial(kernel, devices, capacity, top),
        out_shape=pltpu.VMEM((rows, width), bf16),
        in_specs=[hbm] * 7,
        out_specs=pl.BlockSpec(memory_space=pltpu.VMEM),
        scratch_shapes=[
            pltpu.VMEM((1, width), jnp.float32),
            pltpu.VMEM((top, rows), jnp.int32),
            pltpu.VMEM((top, rows), jnp.float32),
            pltpu.VMEM((2 * top, rows), jnp.float32),
            pltpu.VMEM((3, CHUNKS, rows, step), bf16),
            pltpu.VMEM((3, 2 * top, rows), jnp.float32),
            pltpu.VMEM((3, 2 * unit, rows), bf16),
            pltpu.VMEM((3, rows, 2 * unit), bf16),
            pltpu.VMEM((unit, rows), bf16),
            pltpu.VMEM((rows, unit), bf16),
            pltpu.VMEM((3, CHUNKS, 2 * unit, step), bf16),
            pltpu.VMEM((CHUNKS, unit, step), bf16),
            pltpu.VMEM((4, CHUNKS, unit, step), bf16),
            pltpu.VMEM((unit, ff), bf16),
            pltpu.VMEM((width, ff), bf16),
            pltpu.VMEM((width, ff), bf16),
            pltpu.VMEM((ff, width), bf16),
            pltpu.VMEM((3, CHUNKS, 2 * unit, step), bf16),
            pltpu.VMEM((CHUNKS, unit, step), bf16),
            pltpu.VMEM((2, CHUNKS, rows, step), bf16),
            pltpu.VMEM((rows, step), jnp.float32),
            dma((8,)),
            dma,
            dma((3,)),
            dma((2,)),
            dma((2 * CHUNKS + CHUNKS // 2 + 1,)),
            dma((2,)),
            dma((4,)),
            dma,
            dma((CHUNKS // 2 + 2 * CHUNKS + 1,)),
            dma,
            dma((1 + 2 * CHUNKS,)),
            dma,
            dma((CHUNKS // 2 + 1 + CHUNKS // 2,)),
            pltpu.SemaphoreType.REGULAR,
        ],
        compiler_params=pltpu.CompilerParams(
            collective_id=0, has_side_effects=True, vmem_limit_bytes=VMEM_BYTES
        ),
    )(tokens, norm_gain[None, :], route_ids.T, route_gates.T, w_gate, w_up, w_down)


def solution(mesh):
    placed = (
        P(("grp", "ep"), None),
        P(),
        P(("grp", "ep"), None),
        P(("grp", "ep"), None),
        P("ep", None, None),
        P("ep", None, None),
        P("ep", None, None),
    )
    return jax.shard_map(
        body, mesh=mesh, in_specs=placed, out_specs=P(("grp", "ep"), None), check_vma=False
    )
```

```python
import functools

import jax
import jax.numpy as jnp
from jax import lax
from jax.experimental import pallas as pl
from jax.experimental.pallas import tpu as pltpu
from jax.sharding import PartitionSpec as P

EPS = 1e-06
CHUNKS = 8
TILE = 256
VMEM_BYTES = 62000000


def dot32(a, b):
    return jnp.dot(a, b, preferred_element_type=jnp.float32)


HOME, ACROSS, BEYOND, NEAR = range(4)


def kernel(
    devices, capacity, top,
    tokens_hbm, gain_hbm, ids_hbm, gates_hbm, gate_hbm, up_hbm, down_hbm,
    mixed,
    gain, route_ids, route_gates, table, far, tables, takes, gives, take_near, give_near, packed, packed_near, arrived, hidden,
    w_gate, w_up, w_down, backs, backs_near, partial_in, local,
    load_sems, table_send, table_recv, far_send, far_recv, go_send, go_recv, back_send, back_recv,
    home_recv, part_send, part_recv, ready,
):
    m = devices // 4
    half = 2 * m
    unit = m * capacity
    _, chunks, rows, step = far.shape
    ff = w_gate.shape[1]
    me = lax.axis_index("ep")
    side = me // half
    plane = me // m
    j = me % m
    q = me % half
    own = plane * m
    hub = (1 + side) * m
    leaf = 3 * side * m
    other_hub = (2 - side) * m + j
    peer = own + (j + 1) % m
    is_hub = plane * (3 - plane) > 0

    barrier = pltpu.get_barrier_semaphore()

    @pl.when(is_hub)
    def _():
        pl.semaphore_signal(barrier, inc=1, device_id={"ep": other_hub})

    def greet(i, carry):
        pl.semaphore_signal(barrier, inc=1, device_id={"ep": leaf + (j + 1 + i) % m})
        return carry

    first_load = pltpu.make_async_copy(tokens_hbm.at[:, pl.ds(0, step)], mixed.at[:, pl.ds(0, step)], load_sems.at[7])
    token_load = pltpu.make_async_copy(
        tokens_hbm.at[:, pl.ds(step, (chunks - 1) * step)],
        mixed.at[:, pl.ds(step, (chunks - 1) * step)],
        load_sems.at[3],
    )
    small_loads = [
        pltpu.make_async_copy(ids_hbm, route_ids, load_sems.at[4]),
        pltpu.make_async_copy(gates_hbm, route_gates, load_sems.at[5]),
        pltpu.make_async_copy(gain_hbm, gain, load_sems.at[6]),
    ]
    first_load.start()
    token_load.start()
    for load in small_loads:
        load.start()
    lax.fori_loop(0, m - 1, greet, 0)

    @pl.when(is_hub)
    def _():
        pl.semaphore_signal(barrier, inc=1, device_id={"ep": leaf + j})

    loads = [
        pltpu.make_async_copy(gate_hbm.at[0], w_gate, load_sems.at[0]),
        pltpu.make_async_copy(up_hbm.at[0], w_up, load_sems.at[1]),
        pltpu.make_async_copy(down_hbm.at[0], w_down, load_sems.at[2]),
    ]
    first_load.wait()

    @pl.when(is_hub)
    def _():
        pl.semaphore_wait(barrier, 1)

    @pl.when(jnp.logical_not(is_hub))
    def _():
        pl.semaphore_wait(barrier, half - 1)

    def remote(src, dst, send, recv, device):
        return pltpu.make_async_remote_copy(
            src_ref=src, dst_ref=dst, send_sem=send, recv_sem=recv, device_id={"ep": device}
        )

    def raw(c):
        return mixed.at[:, pl.ds(pl.multiple_of(c * step, step), step)]

    def table_copy(r, src, device):
        return remote(src, tables.at[r - 1], table_send, table_recv.at[r - 1], device)

    def far_slot(r, c):
        return far_recv.at[2 * chunks + c if r == ACROSS else (r - BEYOND) * chunks + c]

    def far_copy(r, c, src, device, group=None):
        send = far_send.at[1 if r == BEYOND else 0]
        return remote(src, far.at[r - 1, c], send, far_slot(r, c if group is None else group), device)

    def part_slot(slot, c):
        return part_recv.at[c // 2] if slot else far_slot(ACROSS, c // 2 + c // (chunks - 1))

    def part_copy(c, src, slot, device):
        return remote(src.at[c], partial_in.at[slot, c], part_send, part_slot(slot, c), device)

    def part_wait(slot, c, count):
        got = partial_in.at[slot, pl.ds(c, count)]
        remote(got, got, part_send, part_slot(slot, c), peer).wait_recv()

    def span(i, part=0):
        return pl.ds(pl.multiple_of(part * unit + i * capacity, 16), capacity)

    def packs(r, c):
        return packed_near.at[c] if r == NEAR else packed.at[r, c]

    def returns(r, c):
        return backs_near.at[c] if r == NEAR else backs.at[r, c]

    def go_copy(r, c, part, i):
        target = (leaf if part else own) + i
        return remote(
            packs(r, c).at[span(i, part)], arrived.at[r, c, span(j)],
            go_send.at[r // NEAR], go_recv.at[r], target,
        )

    def settle(r, every):
        count = unit if every else unit - capacity
        got = arrived.at[r, :, pl.ds(0, count)]
        remote(got, got, go_send.at[0], go_recv.at[r], peer).wait_recv()

    def go_sent(near):
        sent = packed_near.at[:, pl.ds(0, unit - capacity)] if near else packed.at[:, :, pl.ds(0, 2 * unit - capacity)]
        remote(sent, sent, go_send.at[near], go_recv.at[0], peer).wait_send()

    def back_slot(r, c):
        if r == BEYOND:
            return back_recv.at[c]
        if r == NEAR:
            return back_recv.at[2 * chunks]
        return back_recv.at[chunks + (0 if r == HOME else chunks // 2) + c // 2]

    def back_copy(r, c, i):
        return remote(
            arrived.at[r, c, span(i)], returns(r, c).at[span(j)],
            back_send, back_slot(r, c), own + i,
        )

    def back_sent():
        sent = arrived.at[:, :, pl.ds(0, unit - capacity)]
        remote(sent, sent, back_send, go_recv.at[0], peer).wait_send()

    def relay_slot(r, c):
        if r == HOME:
            return home_recv
        return far_slot(NEAR if r == BEYOND else BEYOND, c)

    def relay_copy(r, c):
        return remote(
            backs.at[r, c, pl.ds(0, unit)], backs.at[r, c, pl.ds(unit, unit)],
            part_send, relay_slot(r, c), hub + j,
        )

    def others(act):
        def one(i, carry):
            act((j + 1 + i) % m)
            return carry

        lax.fori_loop(0, m - 1, one, 0)

    def everyone(act):
        def one(i, carry):
            act((j + i) % m)
            return carry

        lax.fori_loop(0, m, one, 0)

    def matrices(source, take, give, bases):
        width = 128

        def block(part, first):
            def one(i, carry):
                at = pl.multiple_of(part * unit + i * width, width)
                start = first * capacity + i * width
                slots = (start + lax.broadcasted_iota(jnp.int32, (width, rows), 0)).astype(jnp.float32)
                taken = jnp.zeros((width, rows), jnp.float32)
                total = jnp.zeros((width, rows), jnp.float32)
                for k in range(top):
                    hit = source[k : k + 1, :] == slots
                    taken = taken + jnp.where(hit, 1.0, 0.0)
                    total = total + jnp.where(hit, source[top + k : top + k + 1, :], 0.0)
                take[pl.ds(at, width), :] = taken.astype(jnp.bfloat16)
                give[:, pl.ds(at, width)] = total.T.astype(jnp.bfloat16)
                return carry

            lax.fori_loop(0, unit // width, one, 0)

        for part, first in enumerate(bases):
            block(part, first)

    def build_table():
        for load in small_loads:
            load.wait()
        expert_at = lax.broadcasted_iota(jnp.int32, (devices, rows), 0)
        hits = [route_ids[k : k + 1, :] == expert_at for k in range(top)]
        named = sum(jnp.where(h, 1.0, 0.0) for h in hits)
        earlier = lax.broadcasted_iota(jnp.int32, (rows, rows), 0) < lax.broadcasted_iota(jnp.int32, (rows, rows), 1)
        ranked = dot32(named.astype(jnp.bfloat16), jnp.where(earlier, 1.0, 0.0).astype(jnp.bfloat16))
        base = ranked + (expert_at * capacity).astype(jnp.float32)
        gates = route_gates[...]
        weights = gates / jnp.sum(gates, axis=0, keepdims=True)
        for k in range(top):
            table[k : k + 1, :] = jnp.sum(jnp.where(hits[k], base, 0.0), axis=0, keepdims=True)
            table[top + k : top + k + 1, :] = weights[k : k + 1, :]

    def each(low, high, act):
        def one(c, carry):
            act(c)
            return carry

        lax.fori_loop(low, high, one, 0)

    def pack(r, c, source):
        take = take_near if r == NEAR else takes.at[r]
        target = packs(r, c)

        target[...] = dot32(take[...], source[...]).astype(jnp.bfloat16)
        if r != NEAR:
            everyone(lambda i: go_copy(r, c, 1, i).start())
        others(lambda i: go_copy(r, c, 0, i).start())
        arrived[r, c, span(j), :] = target[span(j), :]

    def hand_back(r, c):
        others(lambda i: back_copy(r, c, i).start())
        returns(r, c)[span(j), :] = arrived[r, c, span(j), :]

    def norm(r):
        block = 64

        def some(i, carry):
            at = pl.ds(pl.multiple_of(i * block, block), block)
            total = jnp.zeros((block, 1), jnp.float32)
            for c in range(chunks):
                floats = arrived[r, c, at, :].astype(jnp.float32)
                total += jnp.sum(floats * floats, axis=-1, keepdims=True)
            scale = lax.rsqrt(total / (chunks * step) + EPS)
            for c in range(chunks):
                floats = arrived[r, c, at, :].astype(jnp.float32)
                value = floats * scale * gain[:, c * step : (c + 1) * step]
                arrived[r, c, at, :] = value.astype(jnp.bfloat16)
            return carry

        lax.fori_loop(0, unit // block, some, 0)

    def expert(r, send):
        norm(r)

        def gated(i, carry):
            cols = pl.ds(pl.multiple_of(i * TILE, TILE), TILE)
            gate_pre = dot32(arrived[r, 0], w_gate[0:step, cols])
            up_pre = dot32(arrived[r, 0], w_up[0:step, cols])
            for c in range(1, chunks):
                gate_pre += dot32(arrived[r, c], w_gate[c * step : (c + 1) * step, cols])
                up_pre += dot32(arrived[r, c], w_up[c * step : (c + 1) * step, cols])
            hidden[:, cols] = (gate_pre / (1.0 + jnp.exp(-gate_pre)) * up_pre).astype(jnp.bfloat16)
            return carry

        lax.fori_loop(0, ff // TILE, gated, 0)

        def out(c):
            cols = pl.ds(pl.multiple_of(c * step, step), step)
            arrived[r, c] = dot32(hidden[...], w_down[:, cols]).astype(jnp.bfloat16)
            if send:
                hand_back(r, c)

        each(0, chunks, out)

    def finish(c, total):
        mixed[:, pl.ds(pl.multiple_of(c * step, step), step)] = total.astype(jnp.bfloat16)

    def wait_back(r, c):
        got = returns(r, c).at[pl.ds(0, unit - capacity)]
        remote(got, got, back_send, back_slot(r, c), peer).wait_recv()

    def wait_pair(r, p):
        got = backs.at[r, pl.ds(2 * p, 2), pl.ds(0, unit - capacity)]
        remote(got, got, back_send, back_slot(r, 2 * p), peer).wait_recv()

    def wait_near():
        got = backs_near.at[:, pl.ds(0, unit - capacity)]
        remote(got, got, back_send, back_slot(NEAR, 0), peer).wait_recv()

    def all_sent(sem, ref):
        remote(ref, ref, sem, go_recv.at[0], peer).wait_send()

    def hub_role():
        bases = (hub, leaf)
        lead = 2
        mid = chunks // 2

        def across_out(c, group):
            far_copy(ACROSS, c, raw(c), other_hub, group).start()

        across_out(0, 0)
        token_load.wait()
        build_table()
        table_copy(ACROSS, table, other_hub).start()
        each(1, lead, lambda c: across_out(c, 0))
        for load in loads:
            load.start()
        matrices(table, takes.at[HOME], gives.at[HOME], bases)
        pl.semaphore_wait(ready, m)
        each(0, chunks, lambda c: pack(HOME, c, raw(c)))
        table_copy(NEAR, table, leaf + j).wait_recv()
        table_copy(BEYOND, tables.at[NEAR - 1], other_hub).start()
        matrices(tables.at[NEAR - 1], take_near, give_near, (own,))

        def near_in(c):
            far_copy(NEAR, c, raw(c), leaf + j).wait_recv()
            far_copy(BEYOND, c, far.at[NEAR - 1, c], other_hub).start()
            pack(NEAR, c, far.at[NEAR - 1, c])

        def far_in(r, c):
            far_copy(r, c, raw(c), other_hub).wait_recv()
            pack(r, c, far.at[r - 1, c])

        def merge(r, c):
            if r == BEYOND:
                wait_back(r, c)
            relay_copy(r, c).wait_recv()
            far[r - 1, c] = dot32(gives[r], backs[r, c]).astype(jnp.bfloat16)
            part_copy(c, far.at[r - 1], 0 if r == ACROSS else 1, other_hub).start()

        def merge_pair(p):
            wait_pair(ACROSS, p)
            each(2 * p, 2 * p + 2, lambda c: merge(ACROSS, c))

        def pass_on(p):
            part_wait(1, 2 * p, 2)

            def one(c):
                total = dot32(give_near[...], backs_near[c]) + partial_in[1, c].astype(jnp.float32)
                far[NEAR - 1, c] = total.astype(jnp.bfloat16)
                part_copy(c, far.at[NEAR - 1], 1, leaf + j).start()

            each(2 * p, 2 * p + 2, one)

        def beyond_in(c):
            far_in(BEYOND, c)

        def across_in(low, count, group):
            got = far.at[ACROSS - 1, pl.ds(low, count)]
            remote(got, got, far_send.at[0], far_slot(ACROSS, group), peer).wait_recv()
            each(low, low + count, lambda c: pack(ACROSS, c, far.at[ACROSS - 1, c]))

        def across_one(c):
            across_in(c, 1, c - mid + 1)

        each(0, lead, near_in)
        table_copy(ACROSS, table, other_hub).wait_recv()
        matrices(tables.at[ACROSS - 1], takes.at[ACROSS], gives.at[ACROSS], bases)
        table_copy(BEYOND, table, other_hub).wait_recv()
        matrices(tables.at[BEYOND - 1], takes.at[BEYOND], gives.at[BEYOND], bases)

        def early(c):
            beyond_in(c)
            near_in(c + lead)

        each(0, chunks - lead, early)
        each(lead, mid + 1, lambda c: across_out(c, 1))
        each(mid + 1, chunks, lambda c: across_out(c, c - mid + 1))
        for load in loads:
            load.wait()
        settle(HOME, False)
        expert(HOME, False)
        each(chunks - lead, chunks, beyond_in)
        across_in(0, lead, 0)
        settle(NEAR, False)
        expert(NEAR, False)
        settle(BEYOND, False)
        expert(BEYOND, True)
        across_in(lead, mid + 1 - lead, 1)
        each(mid + 1, chunks - 1, across_one)
        merge(BEYOND, 0)
        across_one(chunks - 1)
        each(0, chunks, lambda c: hand_back(NEAR, c))
        each(1, mid + lead, lambda c: merge(BEYOND, c))
        all_sent(far_send.at[1], far.at[NEAR - 1])
        settle(ACROSS, False)
        expert(ACROSS, True)
        each(mid + lead, chunks, lambda c: merge(BEYOND, c))
        each(0, chunks, lambda c: hand_back(HOME, c))
        wait_near()
        each(0, mid // 2, pass_on)

        def late(p):
            pass_on(p)
            merge_pair(p - mid // 2)

        each(mid // 2, chunks // 2, late)
        each(mid // 2, chunks // 2, merge_pair)
        all_sent(table_send, tables.at[pl.ds(0, 2)])
        all_sent(far_send.at[0], mixed)
        go_sent(0)
        go_sent(1)
        back_sent()
        each(0, chunks // 2, lambda p: wait_pair(HOME, p))
        got = backs.at[HOME, :, pl.ds(0, unit)]
        remote(got, got, part_send, home_recv, peer).wait_recv()

        def close(c, wait):
            local[...] = dot32(gives[HOME], backs[HOME, c])
            wait()
            finish(c, local[...] + partial_in[0, c].astype(jnp.float32))

        def close_pair(p):
            close(2 * p, lambda: part_wait(0, 2 * p, 2))
            close(2 * p + 1, lambda: None)

        each(0, chunks // 2 - 1, close_pair)
        each(chunks - 2, chunks, lambda c: close(c, lambda: part_wait(0, c, 1)))
        all_sent(part_send, far)

    def leaf_role():
        far_copy(NEAR, 0, raw(0), hub + j).start()
        each(0, m, lambda i: pl.semaphore_signal(ready, inc=1, device_id={"ep": hub + (j + i) % m}))
        token_load.wait()
        build_table()
        table_copy(NEAR, table, hub + j).start()
        each(1, chunks, lambda c: far_copy(NEAR, c, raw(c), hub + j).start())
        for load in loads:
            load.start()
        matrices(table, take_near, give_near, (own,))
        for load in loads:
            load.wait()

        def send_on(c):
            wait_back(BEYOND, c)
            relay_copy(BEYOND, c).start()

        def send_pair(r, p):
            wait_pair(r, p)
            each(2 * p, 2 * p + 2, lambda c: relay_copy(r, c).start())

        settle(HOME, True)
        expert(HOME, True)
        each(0, chunks // 2 - 1, lambda p: send_pair(HOME, p))
        settle(BEYOND, True)
        expert(BEYOND, True)
        each(0, chunks, send_on)
        send_pair(HOME, chunks // 2 - 1)
        settle(ACROSS, True)
        expert(ACROSS, True)
        each(0, chunks, lambda c: pack(NEAR, c, raw(c)))
        each(0, chunks // 2, lambda p: send_pair(ACROSS, p))
        settle(NEAR, False)
        expert(NEAR, True)
        all_sent(table_send, table)
        all_sent(far_send.at[0], mixed)

        wait_near()

        def close_pair(p):
            part_wait(1, 2 * p, 2)
            for c in (2 * p, 2 * p + 1):
                finish(c, dot32(give_near[...], backs_near[c]) + partial_in[1, c].astype(jnp.float32))

        each(0, chunks // 2, close_pair)
        go_sent(1)
        back_sent()
        all_sent(part_send, backs.at[:, :, pl.ds(0, unit)])

    @pl.when(is_hub)
    def _():
        hub_role()

    @pl.when(jnp.logical_not(is_hub))
    def _():
        leaf_role()


def body(tokens, norm_gain, route_ids, route_gates, w_gate, w_up, w_down):
    rows, width = tokens.shape
    top = route_ids.shape[1]
    devices = lax.axis_size("ep")
    experts = devices
    ff = w_gate.shape[2]
    capacity = 3 * rows * top // (2 * experts)
    m = devices // 4
    unit = m * capacity
    step = width // CHUNKS
    hbm = pl.BlockSpec(memory_space=pl.ANY)
    bf16 = jnp.bfloat16
    dma = pltpu.SemaphoreType.DMA
    return pl.pallas_call(
        functools.partial(kernel, devices, capacity, top),
        out_shape=pltpu.VMEM((rows, width), bf16),
        in_specs=[hbm] * 7,
        out_specs=pl.BlockSpec(memory_space=pltpu.VMEM),
        scratch_shapes=[
            pltpu.VMEM((1, width), jnp.float32),
            pltpu.VMEM((top, rows), jnp.int32),
            pltpu.VMEM((top, rows), jnp.float32),
            pltpu.VMEM((2 * top, rows), jnp.float32),
            pltpu.VMEM((3, CHUNKS, rows, step), bf16),
            pltpu.VMEM((3, 2 * top, rows), jnp.float32),
            pltpu.VMEM((3, 2 * unit, rows), bf16),
            pltpu.VMEM((3, rows, 2 * unit), bf16),
            pltpu.VMEM((unit, rows), bf16),
            pltpu.VMEM((rows, unit), bf16),
            pltpu.VMEM((3, CHUNKS, 2 * unit, step), bf16),
            pltpu.VMEM((CHUNKS, unit, step), bf16),
            pltpu.VMEM((4, CHUNKS, unit, step), bf16),
            pltpu.VMEM((unit, ff), bf16),
            pltpu.VMEM((width, ff), bf16),
            pltpu.VMEM((width, ff), bf16),
            pltpu.VMEM((ff, width), bf16),
            pltpu.VMEM((3, CHUNKS, 2 * unit, step), bf16),
            pltpu.VMEM((CHUNKS, unit, step), bf16),
            pltpu.VMEM((2, CHUNKS, rows, step), bf16),
            pltpu.VMEM((rows, step), jnp.float32),
            dma((8,)),
            dma,
            dma((3,)),
            dma((2,)),
            dma((2 * CHUNKS + CHUNKS // 2 + 1,)),
            dma((2,)),
            dma((4,)),
            dma,
            dma((2 * CHUNKS + 1,)),
            dma,
            dma,
            dma((CHUNKS // 2,)),
            pltpu.SemaphoreType.REGULAR,
        ],
        compiler_params=pltpu.CompilerParams(
            collective_id=0, has_side_effects=True, vmem_limit_bytes=VMEM_BYTES
        ),
    )(tokens, norm_gain[None, :], route_ids.T, route_gates.T, w_gate, w_up, w_down)


def solution(mesh):
    placed = (
        P(("grp", "ep"), None),
        P(),
        P(("grp", "ep"), None),
        P(("grp", "ep"), None),
        P("ep", None, None),
        P("ep", None, None),
        P("ep", None, None),
    )
    return jax.shard_map(
        body, mesh=mesh, in_specs=placed, out_specs=P(("grp", "ep"), None), check_vma=False
    )
```

```python
import functools

import jax
import jax.numpy as jnp
from jax import lax
from jax.experimental import pallas as pl
from jax.experimental.pallas import tpu as pltpu
from jax.sharding import PartitionSpec as P

EPS = 1e-06
CHUNKS = 8
TILE = 256
VMEM_BYTES = 62000000


def dot32(a, b):
    return jnp.dot(a, b, preferred_element_type=jnp.float32)


HOME, ACROSS, BEYOND, NEAR = range(4)


def kernel(
    devices, capacity, top,
    tokens_hbm, gain_hbm, ids_hbm, gates_hbm, gate_hbm, up_hbm, down_hbm,
    mixed,
    gain, route_ids, route_gates, table, far, tables, takes, gives, take_near, give_near, packed, packed_near, arrived, hidden,
    w_gate, w_up, w_down, backs, backs_near, partial_in, local,
    load_sems, table_send, far_send, far_recv, go_send, go_recv, back_send, back_recv,
    home_recv, part_send, part_recv, ready,
):
    m = devices // 4
    half = 2 * m
    unit = m * capacity
    _, chunks, rows, step = far.shape
    ff = w_gate.shape[1]
    me = lax.axis_index("ep")
    side = me // half
    plane = me // m
    j = me % m
    q = me % half
    own = plane * m
    hub = (1 + side) * m
    leaf = 3 * side * m
    other_hub = (2 - side) * m + j
    peer = own + (j + 1) % m
    is_hub = plane * (3 - plane) > 0

    barrier = pltpu.get_barrier_semaphore()

    @pl.when(is_hub)
    def _():
        pl.semaphore_signal(barrier, inc=1, device_id={"ep": other_hub})

    def greet(i, carry):
        pl.semaphore_signal(barrier, inc=1, device_id={"ep": leaf + (j + 1 + i) % m})
        return carry

    first_load = pltpu.make_async_copy(tokens_hbm.at[:, pl.ds(0, step)], mixed.at[:, pl.ds(0, step)], load_sems.at[4])
    token_load = pltpu.make_async_copy(
        tokens_hbm.at[:, pl.ds(step, (chunks - 1) * step)],
        mixed.at[:, pl.ds(step, (chunks - 1) * step)],
        load_sems.at[0],
    )
    small_loads = [
        pltpu.make_async_copy(ids_hbm, route_ids, load_sems.at[1]),
        pltpu.make_async_copy(gates_hbm, route_gates, load_sems.at[2]),
        pltpu.make_async_copy(gain_hbm, gain, load_sems.at[3]),
    ]
    first_load.start()
    token_load.start()
    for load in small_loads:
        load.start()
    lax.fori_loop(0, m - 1, greet, 0)

    @pl.when(is_hub)
    def _():
        pl.semaphore_signal(barrier, inc=1, device_id={"ep": leaf + j})

    loads = [
        pltpu.make_async_copy(gate_hbm.at[0], w_gate, part_recv.at[0]),
        pltpu.make_async_copy(up_hbm.at[0], w_up, part_recv.at[1]),
        pltpu.make_async_copy(down_hbm.at[0], w_down, part_recv.at[2]),
    ]
    first_load.wait()

    @pl.when(is_hub)
    def _():
        pl.semaphore_wait(barrier, 1)

    @pl.when(jnp.logical_not(is_hub))
    def _():
        pl.semaphore_wait(barrier, half - 1)

    def remote(src, dst, send, recv, device):
        return pltpu.make_async_remote_copy(
            src_ref=src, dst_ref=dst, send_sem=send, recv_sem=recv, device_id={"ep": device}
        )

    def raw(c):
        return mixed.at[:, pl.ds(pl.multiple_of(c * step, step), step)]

    def table_copy(r, src, device):
        return remote(src, tables.at[r - 1], table_send, load_sems.at[5 + r - 1], device)

    def far_slot(r, c):
        return far_recv.at[2 * chunks + c if r == ACROSS else (r - BEYOND) * chunks + c]

    def far_copy(r, c, src, device, group=None):
        send = far_send.at[1 if r == BEYOND else 0]
        return remote(src, far.at[r - 1, c], send, far_slot(r, c if group is None else group), device)

    def part_slot(slot, c):
        return part_recv.at[c // 2] if slot else far_slot(ACROSS, c // 2 + c // (chunks - 1))

    def part_copy(c, src, slot, device):
        return remote(src.at[c], partial_in.at[slot, c], part_send, part_slot(slot, c), device)

    def part_wait(slot, c, count):
        got = partial_in.at[slot, pl.ds(c, count)]
        remote(got, got, part_send, part_slot(slot, c), peer).wait_recv()

    def span(i, part=0):
        return pl.ds(pl.multiple_of(part * unit + i * capacity, 16), capacity)

    def packs(r, c):
        return packed_near.at[c] if r == NEAR else packed.at[r, c]

    def returns(r, c):
        return backs_near.at[c] if r == NEAR else backs.at[r, c]

    def go_copy(r, c, part, i):
        target = (leaf if part else own) + i
        return remote(
            packs(r, c).at[span(i, part)], arrived.at[r, c, span(j)],
            go_send.at[r // NEAR], go_recv.at[r], target,
        )

    def settle(r, every):
        count = unit if every else unit - capacity
        got = arrived.at[r, :, pl.ds(0, count)]
        remote(got, got, go_send.at[0], go_recv.at[r], peer).wait_recv()

    def go_sent(near):
        sent = packed_near.at[:, pl.ds(0, unit - capacity)] if near else packed.at[:, :, pl.ds(0, 2 * unit - capacity)]
        remote(sent, sent, go_send.at[near], go_recv.at[0], peer).wait_send()

    def back_slot(r, c):
        if r == BEYOND:
            return load_sems.at[c]
        if r == NEAR:
            return back_recv.at[chunks]
        return back_recv.at[(0 if r == HOME else chunks // 2) + c // 2]

    def back_copy(r, c, i):
        return remote(
            arrived.at[r, c, span(i)], returns(r, c).at[span(j)],
            back_send, back_slot(r, c), own + i,
        )

    def back_sent():
        sent = arrived.at[:, :, pl.ds(0, unit - capacity)]
        remote(sent, sent, back_send, go_recv.at[0], peer).wait_send()

    def relay_slot(r, c):
        if r == HOME:
            return home_recv
        return far_slot(NEAR if r == BEYOND else BEYOND, c)

    def relay_copy(r, c):
        return remote(
            backs.at[r, c, pl.ds(0, unit)], backs.at[r, c, pl.ds(unit, unit)],
            part_send, relay_slot(r, c), hub + j,
        )

    def others(act):
        def one(i, carry):
            act((j + 1 + i) % m)
            return carry

        lax.fori_loop(0, m - 1, one, 0)

    def everyone(act):
        def one(i, carry):
            act((j + i) % m)
            return carry

        lax.fori_loop(0, m, one, 0)

    def matrices(source, take, give, bases):
        width = 128

        def block(part, first):
            def one(i, carry):
                at = pl.multiple_of(part * unit + i * width, width)
                start = first * capacity + i * width
                slots = (start + lax.broadcasted_iota(jnp.int32, (width, rows), 0)).astype(jnp.float32)
                taken = jnp.zeros((width, rows), jnp.float32)
                total = jnp.zeros((width, rows), jnp.float32)
                for k in range(top):
                    hit = source[k : k + 1, :] == slots
                    taken = taken + jnp.where(hit, 1.0, 0.0)
                    total = total + jnp.where(hit, source[top + k : top + k + 1, :], 0.0)
                take[pl.ds(at, width), :] = taken.astype(jnp.bfloat16)
                give[:, pl.ds(at, width)] = total.T.astype(jnp.bfloat16)
                return carry

            lax.fori_loop(0, unit // width, one, 0)

        for part, first in enumerate(bases):
            block(part, first)

    def build_table():
        for load in small_loads:
            load.wait()
        expert_at = lax.broadcasted_iota(jnp.int32, (devices, rows), 0)
        hits = [route_ids[k : k + 1, :] == expert_at for k in range(top)]
        named = sum(jnp.where(h, 1.0, 0.0) for h in hits)
        earlier = lax.broadcasted_iota(jnp.int32, (rows, rows), 0) < lax.broadcasted_iota(jnp.int32, (rows, rows), 1)
        ranked = dot32(named.astype(jnp.bfloat16), jnp.where(earlier, 1.0, 0.0).astype(jnp.bfloat16))
        base = ranked + (expert_at * capacity).astype(jnp.float32)
        gates = route_gates[...]
        weights = gates / jnp.sum(gates, axis=0, keepdims=True)
        for k in range(top):
            table[k : k + 1, :] = jnp.sum(jnp.where(hits[k], base, 0.0), axis=0, keepdims=True)
            table[top + k : top + k + 1, :] = weights[k : k + 1, :]

    def each(low, high, act):
        def one(c, carry):
            act(c)
            return carry

        lax.fori_loop(low, high, one, 0)

    def pack(r, c, source):
        take = take_near if r == NEAR else takes.at[r]
        target = packs(r, c)

        target[...] = dot32(take[...], source[...]).astype(jnp.bfloat16)
        if r != NEAR:
            everyone(lambda i: go_copy(r, c, 1, i).start())
        others(lambda i: go_copy(r, c, 0, i).start())
        arrived[r, c, span(j), :] = target[span(j), :]

    def hand_back(r, c):
        others(lambda i: back_copy(r, c, i).start())
        returns(r, c)[span(j), :] = arrived[r, c, span(j), :]

    def norm(r):
        block = 64

        def some(i, carry):
            at = pl.ds(pl.multiple_of(i * block, block), block)
            total = jnp.zeros((block, 1), jnp.float32)
            for c in range(chunks):
                floats = arrived[r, c, at, :].astype(jnp.float32)
                total += jnp.sum(floats * floats, axis=-1, keepdims=True)
            scale = lax.rsqrt(total / (chunks * step) + EPS)
            for c in range(chunks):
                floats = arrived[r, c, at, :].astype(jnp.float32)
                value = floats * scale * gain[:, c * step : (c + 1) * step]
                arrived[r, c, at, :] = value.astype(jnp.bfloat16)
            return carry

        lax.fori_loop(0, unit // block, some, 0)

    def expert(r, send):
        norm(r)

        def gated(i, carry):
            cols = pl.ds(pl.multiple_of(i * TILE, TILE), TILE)
            gate_pre = dot32(arrived[r, 0], w_gate[0:step, cols])
            up_pre = dot32(arrived[r, 0], w_up[0:step, cols])
            for c in range(1, chunks):
                gate_pre += dot32(arrived[r, c], w_gate[c * step : (c + 1) * step, cols])
                up_pre += dot32(arrived[r, c], w_up[c * step : (c + 1) * step, cols])
            hidden[:, cols] = (gate_pre / (1.0 + jnp.exp(-gate_pre)) * up_pre).astype(jnp.bfloat16)
            return carry

        lax.fori_loop(0, ff // TILE, gated, 0)

        def out(c):
            cols = pl.ds(pl.multiple_of(c * step, step), step)
            arrived[r, c] = dot32(hidden[...], w_down[:, cols]).astype(jnp.bfloat16)
            if send:
                hand_back(r, c)

        each(0, chunks, out)

    def finish(c, total):
        mixed[:, pl.ds(pl.multiple_of(c * step, step), step)] = total.astype(jnp.bfloat16)

    def wait_back(r, c):
        got = returns(r, c).at[pl.ds(0, unit - capacity)]
        remote(got, got, back_send, back_slot(r, c), peer).wait_recv()

    def wait_pair(r, p):
        got = backs.at[r, pl.ds(2 * p, 2), pl.ds(0, unit - capacity)]
        remote(got, got, back_send, back_slot(r, 2 * p), peer).wait_recv()

    def wait_near():
        got = backs_near.at[:, pl.ds(0, unit - capacity)]
        remote(got, got, back_send, back_slot(NEAR, 0), peer).wait_recv()

    def all_sent(sem, ref):
        remote(ref, ref, sem, go_recv.at[0], peer).wait_send()

    def hub_role():
        bases = (hub, leaf)
        lead = 2
        mid = chunks // 2

        def across_out(c, group):
            far_copy(ACROSS, c, raw(c), other_hub, group).start()

        across_out(0, 0)
        token_load.wait()
        build_table()
        table_copy(ACROSS, table, other_hub).start()
        each(1, lead, lambda c: across_out(c, 0))
        for load in loads:
            load.start()
        matrices(table, takes.at[HOME], gives.at[HOME], bases)
        pl.semaphore_wait(ready, m)
        each(0, chunks, lambda c: pack(HOME, c, raw(c)))
        table_copy(NEAR, table, leaf + j).wait_recv()
        table_copy(BEYOND, tables.at[NEAR - 1], other_hub).start()
        matrices(tables.at[NEAR - 1], take_near, give_near, (own,))

        def near_in(c):
            far_copy(NEAR, c, raw(c), leaf + j).wait_recv()
            far_copy(BEYOND, c, far.at[NEAR - 1, c], other_hub).start()
            pack(NEAR, c, far.at[NEAR - 1, c])

        def far_in(r, c):
            far_copy(r, c, raw(c), other_hub).wait_recv()
            pack(r, c, far.at[r - 1, c])

        def merge(r, c):
            if r == BEYOND:
                wait_back(r, c)
            relay_copy(r, c).wait_recv()
            far[r - 1, c] = dot32(gives[r], backs[r, c]).astype(jnp.bfloat16)
            part_copy(c, far.at[r - 1], 0 if r == ACROSS else 1, other_hub).start()

        def merge_pair(p):
            wait_pair(ACROSS, p)
            each(2 * p, 2 * p + 2, lambda c: merge(ACROSS, c))

        def pass_on(p):
            part_wait(1, 2 * p, 2)

            def one(c):
                total = dot32(give_near[...], backs_near[c]) + partial_in[1, c].astype(jnp.float32)
                far[NEAR - 1, c] = total.astype(jnp.bfloat16)
                part_copy(c, far.at[NEAR - 1], 1, leaf + j).start()

            each(2 * p, 2 * p + 2, one)

        def beyond_in(c):
            far_in(BEYOND, c)

        def across_in(low, count, group):
            got = far.at[ACROSS - 1, pl.ds(low, count)]
            remote(got, got, far_send.at[0], far_slot(ACROSS, group), peer).wait_recv()
            each(low, low + count, lambda c: pack(ACROSS, c, far.at[ACROSS - 1, c]))

        def across_one(c):
            across_in(c, 1, c - mid + 1)

        each(0, lead, near_in)
        table_copy(ACROSS, table, other_hub).wait_recv()
        matrices(tables.at[ACROSS - 1], takes.at[ACROSS], gives.at[ACROSS], bases)
        table_copy(BEYOND, table, other_hub).wait_recv()
        matrices(tables.at[BEYOND - 1], takes.at[BEYOND], gives.at[BEYOND], bases)

        def early(c):
            beyond_in(c)
            near_in(c + lead)

        for load in loads:
            load.wait()
        each(0, chunks - lead, early)
        each(lead, mid + 1, lambda c: across_out(c, 1))
        each(mid + 1, chunks, lambda c: across_out(c, c - mid + 1))
        settle(HOME, False)
        expert(HOME, False)
        each(chunks - lead, chunks, beyond_in)
        across_in(0, lead, 0)
        settle(NEAR, False)
        expert(NEAR, False)
        settle(BEYOND, False)
        expert(BEYOND, True)
        across_in(lead, mid + 1 - lead, 1)
        each(mid + 1, chunks - 1, across_one)
        merge(BEYOND, 0)
        across_one(chunks - 1)
        each(0, chunks, lambda c: hand_back(NEAR, c))
        each(1, mid + lead, lambda c: merge(BEYOND, c))
        all_sent(far_send.at[1], far.at[NEAR - 1])
        settle(ACROSS, False)
        expert(ACROSS, True)
        each(mid + lead, chunks, lambda c: merge(BEYOND, c))
        each(0, chunks, lambda c: hand_back(HOME, c))
        wait_near()
        each(0, mid // 2, pass_on)

        def late(p):
            pass_on(p)
            merge_pair(p - mid // 2)

        each(mid // 2, chunks // 2, late)
        each(mid // 2, chunks // 2, merge_pair)
        all_sent(table_send, tables.at[pl.ds(0, 2)])
        all_sent(far_send.at[0], mixed)
        go_sent(0)
        go_sent(1)
        back_sent()
        each(0, chunks // 2, lambda p: wait_pair(HOME, p))
        got = backs.at[HOME, :, pl.ds(0, unit)]
        remote(got, got, part_send, home_recv, peer).wait_recv()

        def close(c, wait):
            local[...] = dot32(gives[HOME], backs[HOME, c])
            wait()
            finish(c, local[...] + partial_in[0, c].astype(jnp.float32))

        def close_pair(p):
            close(2 * p, lambda: part_wait(0, 2 * p, 2))
            close(2 * p + 1, lambda: None)

        each(0, chunks // 2 - 1, close_pair)
        each(chunks - 2, chunks, lambda c: close(c, lambda: part_wait(0, c, 1)))
        all_sent(part_send, far)

    def leaf_role():
        far_copy(NEAR, 0, raw(0), hub + j).start()
        each(0, m, lambda i: pl.semaphore_signal(ready, inc=1, device_id={"ep": hub + (j + i) % m}))
        token_load.wait()
        build_table()
        table_copy(NEAR, table, hub + j).start()
        each(1, chunks, lambda c: far_copy(NEAR, c, raw(c), hub + j).start())
        for load in loads:
            load.start()
        matrices(table, take_near, give_near, (own,))
        for load in loads:
            load.wait()

        def send_on(c):
            wait_back(BEYOND, c)
            relay_copy(BEYOND, c).start()

        def send_pair(r, p):
            wait_pair(r, p)
            each(2 * p, 2 * p + 2, lambda c: relay_copy(r, c).start())

        settle(HOME, True)
        expert(HOME, True)
        each(0, chunks // 2 - 1, lambda p: send_pair(HOME, p))
        settle(BEYOND, True)
        expert(BEYOND, True)
        each(0, chunks, send_on)
        send_pair(HOME, chunks // 2 - 1)
        settle(ACROSS, True)
        expert(ACROSS, True)
        each(0, chunks, lambda c: pack(NEAR, c, raw(c)))
        each(0, chunks // 2, lambda p: send_pair(ACROSS, p))
        settle(NEAR, False)
        expert(NEAR, True)
        all_sent(table_send, table)
        all_sent(far_send.at[0], mixed)

        wait_near()

        def close_pair(p):
            part_wait(1, 2 * p, 2)
            for c in (2 * p, 2 * p + 1):
                finish(c, dot32(give_near[...], backs_near[c]) + partial_in[1, c].astype(jnp.float32))

        each(0, chunks // 2, close_pair)
        go_sent(1)
        back_sent()
        all_sent(part_send, backs.at[:, :, pl.ds(0, unit)])

    @pl.when(is_hub)
    def _():
        hub_role()

    @pl.when(jnp.logical_not(is_hub))
    def _():
        leaf_role()


def body(tokens, norm_gain, route_ids, route_gates, w_gate, w_up, w_down):
    rows, width = tokens.shape
    top = route_ids.shape[1]
    devices = lax.axis_size("ep")
    experts = devices
    ff = w_gate.shape[2]
    capacity = 3 * rows * top // (2 * experts)
    m = devices // 4
    unit = m * capacity
    step = width // CHUNKS
    hbm = pl.BlockSpec(memory_space=pl.ANY)
    bf16 = jnp.bfloat16
    dma = pltpu.SemaphoreType.DMA
    return pl.pallas_call(
        functools.partial(kernel, devices, capacity, top),
        out_shape=pltpu.VMEM((rows, width), bf16),
        in_specs=[hbm] * 7,
        out_specs=pl.BlockSpec(memory_space=pltpu.VMEM),
        scratch_shapes=[
            pltpu.VMEM((1, width), jnp.float32),
            pltpu.VMEM((top, rows), jnp.int32),
            pltpu.VMEM((top, rows), jnp.float32),
            pltpu.VMEM((2 * top, rows), jnp.float32),
            pltpu.VMEM((3, CHUNKS, rows, step), bf16),
            pltpu.VMEM((3, 2 * top, rows), jnp.float32),
            pltpu.VMEM((3, 2 * unit, rows), bf16),
            pltpu.VMEM((3, rows, 2 * unit), bf16),
            pltpu.VMEM((unit, rows), bf16),
            pltpu.VMEM((rows, unit), bf16),
            pltpu.VMEM((3, CHUNKS, 2 * unit, step), bf16),
            pltpu.VMEM((CHUNKS, unit, step), bf16),
            pltpu.VMEM((4, CHUNKS, unit, step), bf16),
            pltpu.VMEM((unit, ff), bf16),
            pltpu.VMEM((width, ff), bf16),
            pltpu.VMEM((width, ff), bf16),
            pltpu.VMEM((ff, width), bf16),
            pltpu.VMEM((3, CHUNKS, 2 * unit, step), bf16),
            pltpu.VMEM((CHUNKS, unit, step), bf16),
            pltpu.VMEM((2, CHUNKS, rows, step), bf16),
            pltpu.VMEM((rows, step), jnp.float32),
            dma((max(8, CHUNKS),)),
            dma,
            dma((2,)),
            dma((2 * CHUNKS + CHUNKS // 2 + 1,)),
            dma((2,)),
            dma((4,)),
            dma,
            dma((CHUNKS + 1,)),
            dma,
            dma,
            dma((CHUNKS // 2,)),
            pltpu.SemaphoreType.REGULAR,
        ],
        compiler_params=pltpu.CompilerParams(
            collective_id=0, has_side_effects=True, vmem_limit_bytes=VMEM_BYTES
        ),
    )(tokens, norm_gain[None, :], route_ids.T, route_gates.T, w_gate, w_up, w_down)


def solution(mesh):
    placed = (
        P(("grp", "ep"), None),
        P(),
        P(("grp", "ep"), None),
        P(("grp", "ep"), None),
        P("ep", None, None),
        P("ep", None, None),
        P("ep", None, None),
    )
    return jax.shard_map(
        body, mesh=mesh, in_specs=placed, out_specs=P(("grp", "ep"), None), check_vma=False
    )
```
